128 devices in a mesh: st: 64 (over z, y, x), tp: 2 (over core).
Axes of the slice: x: 4, y: 4, z: 4, core: 2. Of those that a mesh axis runs over, the one named last changes fastest.
Arguments:
- tokens: bfloat16 [65536, 2048], P('st'), may hold values from -6 to 6
- store: bfloat16 [256, 64, 2048], P('st'), may hold values from -6 to 6
- passage_ids: int32 [1024, 4], P('st'), may hold values from 0 to 255, as said below
- w_query: bfloat16 [2048, 2048], P(None, 'tp'), may hold values from -0.125 to 0.125
- w_key: bfloat16 [2048, 512], P(None, 'tp'), may hold values from -0.125 to 0.125
- w_value: bfloat16 [2048, 512], P(None, 'tp'), may hold values from -0.125 to 0.125
- w_ret_query: bfloat16 [2048, 1024], P(None, 'tp'), may hold values from -0.125 to 0.125
- w_ret_key: bfloat16 [2048, 1024], P(None, 'tp'), may hold values from -0.125 to 0.125
- w_ret_value: bfloat16 [2048, 2048], P(None, 'tp'), may hold values from -0.125 to 0.125
- ret_rate: float32 [8], P('tp'), may hold values from 0.003 to 0.03
- ret_gain: float32 [2048], P('tp'), may hold values from 0.1 to 1.9
- gate_logit: float32 [2048], P('tp'), may hold values from -2 to 2
- out_grad: bfloat16 [65536, 2048], P('st', 'tp'), may hold values from -6 to 6
Outputs:
- grad_tokens: bfloat16 [65536, 2048], P(('st', 'tp'))
- grad_store: bfloat16 [256, 64, 2048], P(('st', 'tp'))
- grad_key_weight: float32 [2048, 512], P(None, 'tp')
The draws below stay inside these ranges and needn't reach their ends.
Inputs may be any that keep to these rules, and one draw needn't show every extreme that they name: `passage_ids`: passage p lies on index p // 4 of st. The rows of one device name exactly 1 passage of every owner, so the 4 passages of a block differ.
All inputs are finite; a program needn't handle non-finite values.
Results may differ from the reference program's by a relative error of at most 0.012.
Values may be sent and summed in bfloat16 or wider, within the bound.
A program may use at most 192 MiB of HBM per device.

```python
import math
import jax
import jax.numpy as jnp
from jax import lax

D = 2048
HEADS = 8
HEAD = 256
KV_HEADS = 2
RET_HEADS = 8
RET_KEY = 128
RET_VALUE = 256
BLK = 64
KP = 4
PLEN = 64
PASS_DEV = 4
TOK_DEV = 1024
TOKENS = 65536
BLOCKS = 1024
PASSAGES = 256
N_ST = 64


def draw_passage_ids(key, part):

    def for_reader(reader):
        stream = jax.random.fold_in(jax.random.fold_in(key, 7), reader)
        first, second, third = jax.random.split(stream, 3)
        owner = jax.random.permutation(first, N_ST).astype(jnp.int32)
        local = jnp.minimum(jax.random.randint(second, (N_ST,), 0, PASS_DEV), jax.random.randint(third, (N_ST,), 0, PASS_DEV))
        return (owner * PASS_DEV + local).astype(jnp.int32)
    every = jax.vmap(for_reader)(jnp.arange(N_ST, dtype=jnp.int32))
    return every.reshape(BLOCKS, KP)


def shard_levels(own_key, dims, pieces, least, top_value):
    gain = 1.0
    for axis_at, blocks in pieces:
        steps = jax.random.uniform(jax.random.fold_in(jax.random.fold_in(own_key, 6), axis_at), (blocks,), jnp.float32, least / len(pieces), top_value / len(pieces))
        gain = gain * jnp.repeat(jnp.exp(steps), dims[axis_at] // blocks).reshape((-1,) + (1,) * (len(dims) - 1 - axis_at))
    return gain


def scatter_about(rng, extent, spread, bound, pieces=(), kind=jnp.bfloat16):
    values = jax.random.normal(rng, extent, jnp.float32) * spread
    if len(pieces) > 0:
        values = shard_levels(rng, extent, pieces, -0.22, 0.18) * values
    return jnp.clip(values, min=-bound, max=bound).astype(kind)


def setup_inputs(seed: int = 0) -> dict:
    key_list = jax.random.split(jax.random.key(seed), 14)
    tokens = scatter_about(key_list[0], (TOKENS, D), 1.0, 6.0, ((0, 64),))
    store = scatter_about(key_list[1], (PASSAGES, PLEN, D), 1.0, 6.0, ((0, 64),))
    passage_ids = draw_passage_ids(jax.random.fold_in(key_list[13], 71), 0)
    w_query = scatter_about(key_list[3], (D, HEADS * HEAD), D ** -0.5, 0.125, ((1, 2),))
    w_key = scatter_about(key_list[4], (D, KV_HEADS * HEAD), D ** -0.5, 0.125, ((1, 2),))
    w_value = scatter_about(key_list[5], (D, KV_HEADS * HEAD), D ** -0.5, 0.125, ((1, 2),))
    w_ret_query = scatter_about(key_list[6], (D, RET_HEADS * RET_KEY), D ** -0.5, 0.125, ((1, 2),))
    w_ret_key = scatter_about(key_list[7], (D, RET_HEADS * RET_KEY), D ** -0.5, 0.125, ((1, 2),))
    w_ret_value = scatter_about(key_list[8], (D, RET_HEADS * RET_VALUE), D ** -0.5, 0.125, ((1, 2),))
    ret_rate = jnp.clip(jnp.exp(math.log(0.03) - 2.3025851 * jax.random.uniform(key_list[9], (RET_HEADS,), jnp.float32) ** shard_levels(key_list[9], (RET_HEADS,), ((0, 2),), -0.2, 0.2)), 0.003, 0.03)
    ret_gain = jnp.clip(1.0 + 0.18 * jax.random.normal(key_list[10], (D,), jnp.float32), 0.1, 1.9)
    gate_logit = jnp.clip(jax.random.uniform(key_list[11], (D,), jnp.float32, -2.0, 2.0) * shard_levels(key_list[11], (D,), ((0, 2),), -0.4, 0.0), -2.0, 2.0)
    out_grad = scatter_about(key_list[12], (TOKENS, D), 1.0, 6.0, ((0, 64), (1, 2)))
    return {"tokens": tokens, "store": store, "passage_ids": passage_ids, "w_query": w_query, "w_key": w_key, "w_value": w_value, "w_ret_query": w_ret_query, "w_ret_key": w_ret_key, "w_ret_value": w_ret_value, "ret_rate": ret_rate, "ret_gain": ret_gain, "gate_logit": gate_logit, "out_grad": out_grad}


EPSILON = 1.0
HIGH = lax.Precision.HIGHEST

def rounded(values):
    return lax.optimization_barrier(values.astype(jnp.bfloat16)).astype(jnp.float32)

def retention_grads(query_rows, key_rows, value_rows, rates, gains, cotangent):
    length = query_rows.shape[0]
    heads = rates.shape[0]
    queries = query_rows.astype(jnp.float32).reshape(length, heads, -1)
    keyset = key_rows.astype(jnp.float32).reshape(length, heads, -1)
    values = value_rows.astype(jnp.float32).reshape(length, heads, -1)
    positions = jnp.arange(length, dtype=jnp.float32)
    distance = positions[:, None] - positions[None, :]
    damping = jnp.where(distance >= 0.0, jnp.exp(-rates[:, None, None] * jnp.maximum(distance, 0.0)), 0.0) * queries.shape[-1] ** (-0.5)
    raw = jnp.einsum('thd,shd->hts', queries, keyset, precision=HIGH)
    weights = rounded(raw * damping)
    mixed = jnp.einsum('hts,she->the', weights, values, precision=HIGH)
    inverse = lax.rsqrt(lax.optimization_barrier(jnp.mean(mixed * mixed, axis=-1, keepdims=True)) + EPSILON)
    scaled = cotangent.astype(jnp.float32).reshape(length, heads, -1) * gains.reshape(heads, -1)
    inner = lax.optimization_barrier(jnp.mean(scaled * mixed, axis=-1, keepdims=True))
    grad_mixed = rounded(inverse * scaled - inverse * inverse * inverse * mixed * inner)
    grad_weights = rounded(jnp.einsum('the,she->hts', grad_mixed, values, precision=HIGH) * damping)
    grad_first = jnp.einsum('hts,shd->thd', grad_weights, keyset, precision=HIGH).astype(jnp.bfloat16).reshape(length, -1)
    grad_second = jnp.einsum('hts,thd->shd', grad_weights, queries, precision=HIGH).astype(jnp.bfloat16).reshape(length, -1)
    grad_third = jnp.einsum('hts,the->she', weights, grad_mixed, precision=HIGH).astype(jnp.bfloat16).reshape(length, -1)
    return (grad_first, grad_second, grad_third)

def reference(tokens, store, passage_ids, w_query, w_key, w_value, w_ret_query, w_ret_key, w_ret_value, ret_rate, ret_gain, gate_logit, out_grad):
    count, plen, width = store.shape
    kv_width = w_key.shape[1]
    kv_heads = kv_width // HEAD
    group = w_query.shape[1] // HEAD // kv_heads
    flat_store = store.reshape(count * plen, width)
    key_table = jnp.dot(flat_store, w_key, preferred_element_type=jnp.float32).astype(jnp.bfloat16).reshape(count, plen, kv_width)
    value_table = jnp.dot(flat_store, w_value, preferred_element_type=jnp.float32).astype(jnp.bfloat16).reshape(count, plen, kv_width)
    gate = jax.nn.sigmoid(gate_logit)
    blocks_dev = TOK_DEV // BLK
    seq_tokens = tokens.reshape(N_ST, TOK_DEV, width)
    seq_ids = passage_ids.reshape(N_ST, blocks_dev * KP)
    seq_grad = out_grad.reshape(N_ST, TOK_DEV, width)
    factor = HEAD ** (-0.5)

    def per_sequence(carry, inputs):
        rows, ids, grad_rows = inputs
        query_bf = jnp.dot(rows, w_query, preferred_element_type=jnp.float32).astype(jnp.bfloat16)
        keys = key_table[ids].reshape(blocks_dev, KP * plen, kv_heads, HEAD).astype(jnp.float32)
        values = value_table[ids].reshape(blocks_dev, KP * plen, kv_heads, HEAD).astype(jnp.float32)
        queries = query_bf.reshape(blocks_dev, BLK, kv_heads, group, HEAD).astype(jnp.float32)
        scores = jnp.einsum('btkgd,bskd->bkgts', queries, keys, precision=HIGH) * factor
        expo = jnp.exp(scores)
        probs = expo / lax.optimization_barrier(jnp.sum(expo, axis=-1, keepdims=True))
        probs_bf = rounded(probs)
        attn = jnp.einsum('bkgts,bskd->btkgd', probs_bf, values, precision=HIGH)
        grad_attn = grad_rows.astype(jnp.float32).reshape(blocks_dev, BLK, kv_heads, group, HEAD) * gate.reshape(kv_heads, group, HEAD)
        grad_attn_bf = rounded(grad_attn)
        grad_probs = jnp.einsum('btkgd,bskd->bkgts', grad_attn_bf, values, precision=HIGH)
        delta = jnp.einsum('btkgd,btkgd->bkgt', grad_attn, attn, precision=HIGH)
        grad_scores = rounded(probs * (grad_probs - delta[..., None]) * factor)
        grad_query = jnp.einsum('bkgts,bskd->btkgd', grad_scores, keys, precision=HIGH).astype(jnp.bfloat16).reshape(TOK_DEV, -1)
        grad_keys = jnp.einsum('bkgts,btkgd->bskd', grad_scores, queries, precision=HIGH).astype(jnp.bfloat16).reshape(blocks_dev * KP, plen, kv_width)
        grad_values = jnp.einsum('bkgts,btkgd->bskd', probs_bf, grad_attn_bf, precision=HIGH).astype(jnp.bfloat16).reshape(blocks_dev * KP, plen, kv_width)
        ret_query = jnp.dot(rows, w_ret_query, preferred_element_type=jnp.float32).astype(jnp.bfloat16)
        ret_key = jnp.dot(rows, w_ret_key, preferred_element_type=jnp.float32).astype(jnp.bfloat16)
        ret_value = jnp.dot(rows, w_ret_value, preferred_element_type=jnp.float32).astype(jnp.bfloat16)
        grad_rq, grad_rk, grad_rv = retention_grads(ret_query, ret_key, ret_value, ret_rate, ret_gain, grad_rows)
        grad_rows_out = (jnp.dot(grad_query, w_query.T, preferred_element_type=jnp.float32) + jnp.dot(grad_rq, w_ret_query.T, preferred_element_type=jnp.float32) + jnp.dot(grad_rk, w_ret_key.T, preferred_element_type=jnp.float32) + jnp.dot(grad_rv, w_ret_value.T, preferred_element_type=jnp.float32)).astype(jnp.bfloat16)
        slot_rows = store[ids].reshape(-1, width)
        carry = carry + jnp.dot(slot_rows.T, grad_keys.reshape(-1, kv_width), preferred_element_type=jnp.float32)
        return (carry, (grad_rows_out, grad_keys, grad_values))
    start = jnp.zeros((width, kv_width), jnp.float32)
    key_weight_grad, outputs = lax.scan(per_sequence, start, (seq_tokens, seq_ids, seq_grad))
    grad_rows_all, slot_keys, slot_values = outputs
    flat_ids = passage_ids.reshape(-1).astype(jnp.int32)
    passage_keys = jax.ops.segment_sum(slot_keys.reshape(-1, plen * kv_width).astype(jnp.float32), flat_ids, num_segments=count)
    passage_values = jax.ops.segment_sum(slot_values.reshape(-1, plen * kv_width).astype(jnp.float32), flat_ids, num_segments=count)
    keys_bf = passage_keys.astype(jnp.bfloat16).reshape(count * plen, kv_width)
    values_bf = passage_values.astype(jnp.bfloat16).reshape(count * plen, kv_width)
    grad_store = (jnp.dot(keys_bf, w_key.T, preferred_element_type=jnp.float32) + jnp.dot(values_bf, w_value.T, preferred_element_type=jnp.float32)).astype(jnp.bfloat16).reshape(count, plen, width)
    return (grad_rows_all.reshape(-1, width), grad_store, key_weight_grad)
```

```python
import jax
import jax.numpy as jnp
from jax import lax
from jax.sharding import PartitionSpec as P
from jax.experimental import pallas as pl
from jax.experimental.pallas import tpu as pltpu


HEAD = 256
BLK = 64
KP = 4
MOST = 1


EPSILON = 1.0
MESH = pl.DeviceIdType.MESH
STRIDES = (1, 4, 16)
PARTS = ((0, 768), (768, 768), (1536, 512))


def coordinate(me, dim):
    return lax.rem(me // STRIDES[dim], 4)


def peer_of(me, dim, step):
    at = coordinate(me, dim)
    return me + (lax.rem(at + step, 4) - at) * STRIDES[dim]


def line_barrier(me):
    barrier = pltpu.get_barrier_semaphore()
    for dim in range(3):
        for step in (1, 2, 3):
            pl.semaphore_signal(
                barrier, inc=1, device_id={"st": peer_of(me, dim, step)}, device_id_type=MESH
            )
    pl.semaphore_wait(barrier, 9)


def rows_at(start, size):
    return pl.ds(pl.multiple_of(start, 16), size)


def all_reduce_kernel(x_ref, o_ref, half, total, first_in, second_in, third_in, out, send, recv):
    me = lax.axis_index("st")
    line_barrier(me)

    def copy(stage, part, step, dim, source, target):
        return pltpu.make_async_remote_copy(
            src_ref=source,
            dst_ref=target,
            send_sem=send.at[stage, part, step - 1],
            recv_sem=recv.at[stage, part, step - 1],
            device_id={"st": peer_of(me, dim, step)},
            device_id_type=MESH,
        )

    half[...] = x_ref[...].astype(jnp.bfloat16)
    started = []
    for part, (start, size) in enumerate(PARTS):
        dim = part
        at = coordinate(me, dim)
        for step in (1, 2, 3):
            there = lax.rem(at + step, 4)
            quarter = size // 4
            one = copy(
                0,
                part,
                step,
                dim,
                half.at[rows_at(start + there * quarter, quarter)],
                first_in.at[step - 1, pl.ds(start // 4, quarter)],
            )
            one.start()
            started.append(one)
    stage = []
    for part, (start, size) in enumerate(PARTS):
        dim, other = part, (part + 1) % 3
        at, beside = coordinate(me, dim), coordinate(me, other)
        quarter, small = size // 4, size // 16
        base = start + at * quarter
        for step in (1, 2, 3):
            started[part * 3 + step - 1].wait_recv()
        mine = x_ref[rows_at(base, quarter), :]
        for step in (1, 2, 3):
            mine = mine + first_in[step - 1, pl.ds(start // 4, quarter), :].astype(jnp.float32)
        for step in (1, 2, 3):
            started[part * 3 + step - 1].wait_send()
        total[pl.ds(start // 4, quarter), :] = mine
        half[rows_at(base, quarter), :] = mine.astype(jnp.bfloat16)
        for step in (1, 2, 3):
            there = lax.rem(beside + step, 4)
            one = copy(
                1,
                part,
                step,
                other,
                half.at[rows_at(base + there * small, small)],
                second_in.at[step - 1, pl.ds(start // 16, small)],
            )
            one.start()
            stage.append(one)
    started, stage = stage, []
    for part, (start, size) in enumerate(PARTS):
        dim, other, last = part, (part + 1) % 3, (part + 2) % 3
        at, beside = coordinate(me, dim), coordinate(me, other)
        quarter, small = size // 4, size // 16
        base = start + at * quarter + beside * small
        for step in (1, 2, 3):
            started[part * 3 + step - 1].wait_recv()
        mine = total[rows_at(start // 4 + beside * small, small), :]
        for step in (1, 2, 3):
            mine = mine + second_in[step - 1, pl.ds(start // 16, small), :].astype(jnp.float32)
        for step in (1, 2, 3):
            started[part * 3 + step - 1].wait_send()
        total[rows_at(start // 4 + beside * small, small), :] = mine
        half[rows_at(base, small), :] = mine.astype(jnp.bfloat16)
        for step in (1, 2, 3):
            one = copy(
                2,
                part,
                step,
                last,
                half.at[rows_at(base, small)],
                third_in.at[step - 1, pl.ds(start // 16, small)],
            )
            one.start()
            stage.append(one)
    started, stage = stage, []
    for part, (start, size) in enumerate(PARTS):
        dim, other = part, (part + 1) % 3
        at, beside = coordinate(me, dim), coordinate(me, other)
        quarter, small = size // 4, size // 16
        base = start + at * quarter + beside * small
        for step in (1, 2, 3):
            started[part * 3 + step - 1].wait_recv()
        rows = pl.ds(start // 16, small)
        mine = half[rows_at(base, small), :].astype(jnp.float32) + third_in[1, rows, :].astype(
            jnp.float32
        )
        mine = mine + (
            third_in[0, rows, :].astype(jnp.float32) + third_in[2, rows, :].astype(jnp.float32)
        )
        out[rows_at(base, small), :] = mine.astype(jnp.bfloat16)
        for step in (1, 2, 3):
            started[part * 3 + step - 1].wait_send()
        for step in (1, 2, 3):
            one = copy(3, part, step, other, out.at[rows_at(base, small)], out.at[rows_at(base, small)])
            one.start()
            stage.append(one)
    started, stage = stage, []
    for part, (start, size) in enumerate(PARTS):
        dim = part
        at = coordinate(me, dim)
        quarter = size // 4
        base = start + at * quarter
        for step in (1, 2, 3):
            started[part * 3 + step - 1].wait()
        for step in (1, 2, 3):
            one = copy(
                4, part, step, dim, out.at[rows_at(base, quarter)], out.at[rows_at(base, quarter)]
            )
            one.start()
            stage.append(one)
    for one in stage:
        one.wait()
    o_ref[...] = out[...].astype(jnp.float32)


def all_reduce(x):
    rows, width = x.shape
    return pl.pallas_call(
        all_reduce_kernel,
        name="sum_over_st",
        out_shape=jax.ShapeDtypeStruct((rows, width), jnp.float32),
        in_specs=[pl.BlockSpec(memory_space=pltpu.VMEM)],
        out_specs=pl.BlockSpec(memory_space=pltpu.VMEM),
        scratch_shapes=[
            pltpu.VMEM((rows, width), jnp.bfloat16),
            pltpu.VMEM((rows // 4, width), jnp.float32),
            pltpu.VMEM((3, rows // 4, width), jnp.bfloat16),
            pltpu.VMEM((3, rows // 16, width), jnp.bfloat16),
            pltpu.VMEM((3, rows // 16, width), jnp.bfloat16),
            pltpu.VMEM((rows, width), jnp.bfloat16),
            pltpu.SemaphoreType.DMA((5, 3, 3)),
            pltpu.SemaphoreType.DMA((5, 3, 3)),
        ],
        compiler_params=pltpu.CompilerParams(collective_id=0, has_side_effects=True),
    )(x)


def retention_grads(query_rows, key_rows, value_rows, rates, gains, cotangent):
    length = query_rows.shape[0]
    heads = rates.shape[0]
    queries = query_rows.reshape(length, heads, -1)
    keyset = key_rows.reshape(length, heads, -1)
    values = value_rows.reshape(length, heads, -1)
    positions = jnp.arange(length, dtype=jnp.float32)
    distance = positions[:, None] - positions[None, :]
    damping = jnp.where(
        distance >= 0.0, jnp.exp(-rates[:, None, None] * jnp.maximum(distance, 0.0)), 0.0
    ) * queries.shape[-1] ** (-0.5)
    raw = jnp.einsum("thd,shd->hts", queries, keyset, preferred_element_type=jnp.float32)
    weights = (raw * damping).astype(jnp.bfloat16)
    mixed = jnp.einsum("hts,she->the", weights, values, preferred_element_type=jnp.float32)
    inverse = lax.rsqrt(jnp.mean(mixed * mixed, axis=-1, keepdims=True) + EPSILON)
    scaled = cotangent.astype(jnp.float32).reshape(length, heads, -1) * gains.reshape(heads, -1)
    inner = jnp.mean(scaled * mixed, axis=-1, keepdims=True)
    grad_mixed = (inverse * scaled - inverse * inverse * inverse * mixed * inner).astype(
        jnp.bfloat16
    )
    grad_weights = (
        jnp.einsum("the,she->hts", grad_mixed, values, preferred_element_type=jnp.float32) * damping
    ).astype(jnp.bfloat16)
    grad_first = (
        jnp.einsum("hts,shd->thd", grad_weights, keyset, preferred_element_type=jnp.float32)
        .astype(jnp.bfloat16)
        .reshape(length, -1)
    )
    grad_second = (
        jnp.einsum("hts,thd->shd", grad_weights, queries, preferred_element_type=jnp.float32)
        .astype(jnp.bfloat16)
        .reshape(length, -1)
    )
    grad_third = (
        jnp.einsum("hts,the->she", weights, grad_mixed, preferred_element_type=jnp.float32)
        .astype(jnp.bfloat16)
        .reshape(length, -1)
    )
    return (grad_first, grad_second, grad_third)


def against_rows(left, weight):
    return lax.dot_general(
        left, weight, (((1,), (1,)), ((), ())), preferred_element_type=jnp.float32
    )


def across_rows(left, right):
    return lax.dot_general(
        left, right, (((0,), (0,)), ((), ())), preferred_element_type=jnp.float32
    )


def per_device(
    tokens,
    store,
    passage_ids,
    w_query,
    w_key,
    w_value,
    w_ret_query,
    w_ret_key,
    w_ret_value,
    ret_rate,
    ret_gain,
    gate_logit,
    out_grad,
):
    owners = lax.axis_size("st")
    pass_dev, plen, width = store.shape
    length = tokens.shape[0]
    kv_width = w_key.shape[1]
    kv_local = kv_width // HEAD
    group = w_query.shape[1] // HEAD // kv_local
    blocks = length // BLK
    slot_ids = passage_ids.reshape(-1)
    slot_count = slot_ids.shape[0]
    slot_owner = slot_ids // pass_dev
    slot_local = slot_ids % pass_dev
    order = jnp.arange(slot_count, dtype=jnp.int32)
    same_owner = slot_owner[:, None] == slot_owner[None, :]
    rank = jnp.sum(same_owner & (order[None, :] < order[:, None]), axis=1)
    position = slot_owner * MOST + rank
    cells = owners * MOST
    placed = jnp.arange(cells, dtype=jnp.int32)[:, None] == position[None, :]
    request = (jnp.sum(jnp.where(placed, slot_local[None, :] + 1, 0), axis=1) - 1).reshape(
        owners, MOST
    )
    incoming = lax.all_to_all(request, "st", split_axis=0, concat_axis=0, tiled=True)
    wanted = incoming.reshape(-1)
    valid = wanted >= 0
    safe = jnp.maximum(wanted, 0)
    placed_bf = placed.astype(jnp.bfloat16)
    store_rows = store.reshape(-1, width)
    nothing = jnp.zeros((), jnp.bfloat16)
    own_kv = jnp.concatenate(
        [
            jnp.dot(store_rows, w_key, preferred_element_type=jnp.float32).astype(jnp.bfloat16),
            jnp.dot(store_rows, w_value, preferred_element_type=jnp.float32).astype(jnp.bfloat16),
        ],
        axis=1,
    ).reshape(pass_dev, plen, 2 * kv_width)
    reply = jnp.where(valid[:, None, None], own_kv[safe], nothing).reshape(
        owners, MOST, plen, 2 * kv_width
    )
    arrived = lax.all_to_all(reply, "st", split_axis=0, concat_axis=0, tiled=True)
    slot_kv = (
        across_rows(placed_bf, arrived.reshape(cells, -1))
        .astype(jnp.bfloat16)
        .reshape(slot_count, plen, 2 * kv_width)
    )
    factor = HEAD ** (-0.5)
    gate = jax.nn.sigmoid(gate_logit)
    query_bf = jnp.dot(tokens, w_query, preferred_element_type=jnp.float32).astype(jnp.bfloat16)
    queries = query_bf.reshape(blocks, BLK, kv_local, group, HEAD)
    keys = slot_kv[:, :, :kv_width].reshape(blocks, KP * plen, kv_local, HEAD)
    values = slot_kv[:, :, kv_width:].reshape(blocks, KP * plen, kv_local, HEAD)
    scores = (
        jnp.einsum("btkgd,bskd->bkgts", queries, keys, preferred_element_type=jnp.float32) * factor
    )
    expo = jnp.exp(scores)
    probs = expo / jnp.sum(expo, axis=-1, keepdims=True)
    probs_bf = probs.astype(jnp.bfloat16)
    attn = jnp.einsum("bkgts,bskd->btkgd", probs_bf, values, preferred_element_type=jnp.float32)
    grad_attn = out_grad.astype(jnp.float32).reshape(
        blocks, BLK, kv_local, group, HEAD
    ) * gate.reshape(kv_local, group, HEAD)
    grad_attn_bf = grad_attn.astype(jnp.bfloat16)
    grad_probs = jnp.einsum(
        "btkgd,bskd->bkgts", grad_attn_bf, values, preferred_element_type=jnp.float32
    )
    delta = jnp.moveaxis(jnp.sum(grad_attn * attn, axis=-1), 1, 3)
    grad_scores = (probs * (grad_probs - delta[..., None]) * factor).astype(jnp.bfloat16)
    grad_query = (
        jnp.einsum("bkgts,bskd->btkgd", grad_scores, keys, preferred_element_type=jnp.float32)
        .astype(jnp.bfloat16)
        .reshape(length, -1)
    )
    grad_keys = (
        jnp.einsum("bkgts,btkgd->bskd", grad_scores, queries, preferred_element_type=jnp.float32)
        .astype(jnp.bfloat16)
        .reshape(slot_count, plen, kv_width)
    )
    grad_values = (
        jnp.einsum("bkgts,btkgd->bskd", probs_bf, grad_attn_bf, preferred_element_type=jnp.float32)
        .astype(jnp.bfloat16)
        .reshape(slot_count, plen, kv_width)
    )
    slot_grad = jnp.concatenate([grad_keys, grad_values], axis=2)
    outgoing = (
        jnp.dot(placed_bf, slot_grad.reshape(slot_count, -1), preferred_element_type=jnp.float32)
        .astype(jnp.bfloat16)
        .reshape(owners, MOST, plen, 2 * kv_width)
    )
    returned = lax.all_to_all(outgoing, "st", split_axis=0, concat_axis=0, tiled=True)
    matched = (jnp.arange(pass_dev, dtype=jnp.int32)[:, None] == wanted[None, :]).astype(
        jnp.bfloat16
    )
    passage_grad = jnp.dot(
        matched, returned.reshape(cells, -1), preferred_element_type=jnp.float32
    ).reshape(pass_dev * plen, 2 * kv_width)
    key_grad = passage_grad[:, :kv_width]
    upper = key_grad.astype(jnp.bfloat16)
    lower = (key_grad - upper.astype(jnp.float32)).astype(jnp.bfloat16)
    key_term = across_rows(store_rows, upper) + across_rows(store_rows, lower)
    grad_key_weight = all_reduce(key_term)
    passage_bf = passage_grad.astype(jnp.bfloat16)
    grad_store = lax.psum_scatter(
        (
            against_rows(passage_bf[:, :kv_width], w_key)
            + against_rows(passage_bf[:, kv_width:], w_value)
        ).astype(jnp.bfloat16),
        "tp",
        scatter_dimension=0,
        tiled=True,
    ).astype(jnp.float32)
    grad_store = grad_store.astype(jnp.bfloat16).reshape(-1, plen, width)
    ret_query = jnp.dot(tokens, w_ret_query, preferred_element_type=jnp.float32).astype(
        jnp.bfloat16
    )
    ret_key = jnp.dot(tokens, w_ret_key, preferred_element_type=jnp.float32).astype(jnp.bfloat16)
    ret_value = jnp.dot(tokens, w_ret_value, preferred_element_type=jnp.float32).astype(
        jnp.bfloat16
    )
    grad_rq, grad_rk, grad_rv = retention_grads(
        ret_query, ret_key, ret_value, ret_rate, ret_gain, out_grad
    )
    total = against_rows(grad_query, w_query)
    total = total + against_rows(grad_rq, w_ret_query)
    total = total + against_rows(grad_rk, w_ret_key)
    grad_tokens = lax.psum_scatter(
        (total + against_rows(grad_rv, w_ret_value)).astype(jnp.bfloat16),
        "tp",
        scatter_dimension=0,
        tiled=True,
    )
    return (grad_tokens, grad_store, grad_key_weight)


def solution(mesh):
    return jax.shard_map(
        per_device,
        mesh=mesh,
        in_specs=(
            P("st", None),
            P("st", None, None),
            P("st", None),
            P(None, "tp"),
            P(None, "tp"),
            P(None, "tp"),
            P(None, "tp"),
            P(None, "tp"),
            P(None, "tp"),
            P("tp"),
            P("tp"),
            P("tp"),
            P("st", "tp"),
        ),
        out_specs=(P(("st", "tp"), None), P(("st", "tp"), None, None), P(None, "tp")),
        check_vma=False,
    )
```

```python
import functools

import jax
import jax.numpy as jnp
from jax import lax
from jax.experimental import pallas as pl
from jax.experimental.pallas import tpu as pltpu
from jax.sharding import PartitionSpec as P

MESH = pl.DeviceIdType.MESH
HEAD = 256
BLK = 64
KP = 4
PLEN = 64
PASS_DEV = 4
OWNERS = 64
RET_KEY = 128
EPSILON = 1.0
VMEM_LIMIT = 60 * 1024 * 1024

STRIDES = (1, 4, 16)
CHANNELS = (
    (0, 0, 3, 0),
    (0, 3, 3, 1),
    (0, 6, 2, 2),
    (1, 0, 2, 0),
    (1, 2, 3, 1),
    (1, 5, 3, 2),
)
KEY_CHANNELS = (0, 1, 2)
VALUE_CHANNELS = (3, 4, 5)
STEPS = (1, 2, 3)
PARTS = ((0, 768), (768, 768), (1536, 512))


def nn(left, right):
    return jnp.dot(left, right, preferred_element_type=jnp.float32)


def nt(left, right):
    return lax.dot_general(
        left, right, (((1,), (1,)), ((), ())), preferred_element_type=jnp.float32
    )


def tn(left, right):
    return lax.dot_general(
        left, right, (((0,), (0,)), ((), ())), preferred_element_type=jnp.float32
    )


def coordinate(index, dim):
    return lax.rem(index // STRIDES[dim], 4)


def peer_of(me, dim, step):
    at = coordinate(me, dim)
    return me + (lax.rem(at + step, 4) - at) * STRIDES[dim]


def lines(turn):
    return turn, (turn + 1) % 3, (turn + 2) % 3


def line_barrier(me, sibling=None):
    barrier = pltpu.get_barrier_semaphore()
    for dim in range(3):
        for step in STEPS:
            pl.semaphore_signal(
                barrier, inc=1, device_id={"st": peer_of(me, dim, step)}, device_id_type=MESH
            )
    if sibling is None:
        pl.semaphore_wait(barrier, 9)
    else:
        pl.semaphore_signal(barrier, inc=1, device_id={"tp": sibling}, device_id_type=MESH)
        pl.semaphore_wait(barrier, 10)


def aligned(start, size, by=16):
    return pl.ds(pl.multiple_of(start, by), size)


def unit_place(unit):
    return (unit // 2) * 16, (unit % 2) * 128


def forward_kernel(
    need_ref,
    rate_ref,
    gain_ref,
    store_any,
    w_key_any,
    w_value_any,
    tokens_any,
    w_rq_any,
    w_rk_any,
    w_rv_any,
    w_q_any,
    grad_any,
    *rest,
):
    arrived = rest[:6]
    asked, q_any, grq_any, grk_any, grv_any = rest[6:11]
    table, outgoing, own = rest[11:17], rest[17:23], rest[23:29]
    (
        store,
        w_key,
        w_value,
        tokens,
        w_rq,
        w_rk,
        w_rv,
        w_q,
        grad,
        rq,
        rk,
        rv,
        q,
        grq,
        grk,
        grv,
        damp,
        weights,
        grad_weights,
        grad_y,
        load,
        leave,
        id_send,
        id_recv,
        send,
        recv,
    ) = rest[29:]
    me = lax.axis_index("st")
    loads = [
        pltpu.make_async_copy(source, target, load.at[at])
        for at, (source, target) in enumerate(
            (
                (store_any, store),
                (w_key_any, w_key),
                (w_value_any, w_value),
                (tokens_any, tokens),
                (w_rq_any, w_rq),
                (w_rk_any, w_rk),
                (w_rv_any, w_rv),
                (grad_any, grad),
                (w_q_any, w_q),
            )
        )
    ]
    for one in loads:
        one.start()
    line_barrier(me)
    names = []
    for dim in range(3):
        for step in STEPS:
            at = dim * 3 + step - 1
            one = pltpu.make_async_remote_copy(
                src_ref=need_ref.at[0],
                dst_ref=asked.at[at],
                send_sem=id_send.at[at],
                recv_sem=id_recv.at[at],
                device_id={"st": peer_of(me, dim, step)},
                device_id_type=MESH,
            )
            one.start()
            names.append(one)

    def remote(stage, channel, step, dim, source, target):
        return pltpu.make_async_remote_copy(
            src_ref=source,
            dst_ref=target,
            send_sem=send.at[stage, channel, step - 1],
            recv_sem=recv.at[stage, channel, step - 1],
            device_id={"st": peer_of(me, dim, step)},
            device_id_type=MESH,
        )

    def own_rows(kind, weight):
        made = nn(store[...], weight[...]).astype(jnp.bfloat16)
        for channel, (which, first, units, turn) in enumerate(CHANNELS):
            if which != kind:
                continue
            one, two, _ = lines(turn)
            at, beside = coordinate(me, one), coordinate(me, two)
            for passage in range(PASS_DEV):
                for unit in range(units):
                    row, column = unit_place(first + unit)
                    row = row + passage * PLEN
                    table[channel][beside, at, passage, unit] = made[
                        row : row + 16, column : column + 128
                    ]

    def first_stage(channels):
        copies = {}
        for channel in channels:
            one, two, _ = lines(CHANNELS[channel][3])
            at, beside = coordinate(me, one), coordinate(me, two)
            here = table[channel].at[beside, at]
            for step in STEPS:
                copies[channel, step] = remote(0, channel, step, one, here, here)
                copies[channel, step].start()
        return copies

    def second_stage(channels, before):
        copies = {}
        for channel in channels:
            _, two, _ = lines(CHANNELS[channel][3])
            for step in STEPS:
                before[channel, step].wait()
            here = table[channel].at[coordinate(me, two)]
            for step in STEPS:
                copies[channel, step] = remote(1, channel, step, two, here, here)
                copies[channel, step].start()
        return copies

    def third_stage(channels, before):
        copies = {}
        for channel in channels:
            one, two, last = lines(CHANNELS[channel][3])
            here = coordinate(me, last)
            for step in STEPS:
                before[channel, step].wait()

            @pl.loop(0, 16)
            def _(at):
                beside, along = at // 4, lax.rem(at, 4)
                owner = along * STRIDES[one] + beside * STRIDES[two] + here * STRIDES[last]
                own[channel][beside, along] = table[channel][beside, along, need_ref[0, 0, owner]]
                for step in STEPS:
                    row = last * 3 + (4 - step) - 1
                    outgoing[channel][step - 1, beside, along] = table[channel][
                        beside, along, asked[row, 0, owner]
                    ]

            for step in STEPS:
                copies[channel, step] = remote(
                    2,
                    channel,
                    step,
                    last,
                    outgoing[channel].at[step - 1],
                    arrived[channel].at[here],
                )
                copies[channel, step].start()
            copies[channel, 0] = pltpu.make_async_copy(
                own[channel], arrived[channel].at[here], leave.at[channel]
            )
            copies[channel, 0].start()
        return copies

    def project(weight, target):
        @pl.loop(0, weight.shape[1] // 256)
        def _(tile):
            columns = aligned(tile * 256, 256, 256)
            target[:, columns] = nn(tokens[...], weight[:, columns]).astype(jnp.bfloat16)

    def retention(start, stop):
        @pl.loop(start, stop)
        def _(head):
            rate = rate_ref[head]
            narrow = aligned(head * RET_KEY, RET_KEY, 128)
            wide = aligned(head * HEAD, HEAD, 256)
            rows = lax.broadcasted_iota(jnp.int32, (256, 256), 0)
            columns = lax.broadcasted_iota(jnp.int32, (256, 256), 1)
            for apart in range(4):
                distance = (rows - columns + 256 * apart).astype(jnp.float32)
                damp[apart] = jnp.where(
                    distance >= 0.0, jnp.exp(-rate * jnp.maximum(distance, 0.0)), 0.0
                ) * RET_KEY ** (-0.5)
            for i in range(4):
                block = pl.ds(i * 256, 256)
                upto = (i + 1) * 256
                for j in range(i + 1):
                    raw = nt(rq[block, narrow], rk[pl.ds(j * 256, 256), narrow])
                    weights[block, pl.ds(j * 256, 256)] = (raw * damp[i - j]).astype(jnp.bfloat16)
                y = nn(weights[block, pl.ds(0, upto)], rv[pl.ds(0, upto), wide])
                inverse = lax.rsqrt(jnp.mean(y * y, axis=1, keepdims=True) + EPSILON)
                scaled = grad[block, wide].astype(jnp.float32) * gain_ref[:, wide]
                inner = jnp.mean(scaled * y, axis=1, keepdims=True)
                grad_y[block, :] = (
                    inverse * scaled - (inverse * inverse * inverse * inner) * y
                ).astype(jnp.bfloat16)
                for j in range(i + 1):
                    raw = nt(grad_y[block, :], rv[pl.ds(j * 256, 256), wide])
                    grad_weights[block, pl.ds(j * 256, 256)] = (raw * damp[i - j]).astype(
                        jnp.bfloat16
                    )
                grq[block, narrow] = nn(
                    grad_weights[block, pl.ds(0, upto)], rk[pl.ds(0, upto), narrow]
                ).astype(jnp.bfloat16)
            for j in range(4):
                block = pl.ds(j * 256, 256)
                after = pl.ds(j * 256, 1024 - j * 256)
                grk[block, narrow] = tn(grad_weights[after, block], rq[after, narrow]).astype(
                    jnp.bfloat16
                )
                grv[block, wide] = tn(weights[after, block], grad_y[after, :]).astype(jnp.bfloat16)

    loads[0].wait()
    loads[1].wait()
    own_rows(0, w_key)
    keys = first_stage(KEY_CHANNELS)
    loads[2].wait()
    own_rows(1, w_value)
    values = first_stage(VALUE_CHANNELS)
    for one in names:
        one.wait()
    loads[3].wait()
    loads[4].wait()
    project(w_rq, rq)
    keys = second_stage(KEY_CHANNELS, keys)
    values = second_stage(VALUE_CHANNELS, values)
    loads[5].wait()
    project(w_rk, rk)
    loads[6].wait()
    project(w_rv, rv)
    loads[7].wait()
    retention(0, 1)
    keys = third_stage(KEY_CHANNELS, keys)
    retention(1, 2)
    values = third_stage(VALUE_CHANNELS, values)
    loads[8].wait()
    project(w_q, q)
    ends = [pltpu.make_async_copy(q, q_any, leave.at[6])]
    ends[0].start()
    retention(2, 4)
    for at, (source, target) in enumerate(((grq, grq_any), (grk, grk_any), (grv, grv_any))):
        one = pltpu.make_async_copy(source, target, leave.at[7 + at])
        one.start()
        ends.append(one)
    for one in list(keys.values()) + list(values.values()) + ends:
        one.wait()


def any_spec():
    return pl.BlockSpec(memory_space=pl.ANY)


def vmem_spec():
    return pl.BlockSpec(memory_space=pltpu.VMEM)


def smem_spec():
    return pl.BlockSpec(memory_space=pltpu.SMEM)


def forward(need, rate, gain, store, w_key, w_value, tokens, w_rq, w_rk, w_rv, w_q, grad):
    bf16, f32 = jnp.bfloat16, jnp.float32
    length, width = tokens.shape
    units = [channel[2] for channel in CHANNELS]
    out_shape = (
        [jax.ShapeDtypeStruct((4, 4, 4, n, 16, 128), bf16) for n in units]
        + [jax.ShapeDtypeStruct((9, 1, 128), jnp.int32)]
        + [
            jax.ShapeDtypeStruct((length, n), bf16)
            for n in (w_q.shape[1], w_rq.shape[1], w_rk.shape[1], w_rv.shape[1])
        ]
    )
    scratch = (
        [pltpu.VMEM((4, 4, 4, n, 16, 128), bf16) for n in units]
        + [pltpu.VMEM((3, 4, 4, n, 16, 128), bf16) for n in units]
        + [pltpu.VMEM((4, 4, n, 16, 128), bf16) for n in units]
        + [
            pltpu.VMEM(array.shape, array.dtype)
            for array in (store, w_key, w_value, tokens, w_rq, w_rk, w_rv, w_q, grad)
        ]
        + [
            pltpu.VMEM((length, n), bf16)
            for n in (w_rq.shape[1], w_rk.shape[1], w_rv.shape[1], w_q.shape[1])
        ]
        + [pltpu.VMEM((length, n), bf16) for n in (w_rq.shape[1], w_rk.shape[1], w_rv.shape[1])]
        + [
            pltpu.VMEM((4, 256, 256), f32),
            pltpu.VMEM((length, length), bf16),
            pltpu.VMEM((length, length), bf16),
            pltpu.VMEM((length, HEAD), bf16),
            pltpu.SemaphoreType.DMA((9,)),
            pltpu.SemaphoreType.DMA((10,)),
            pltpu.SemaphoreType.DMA((9,)),
            pltpu.SemaphoreType.DMA((9,)),
            pltpu.SemaphoreType.DMA((3, 6, 3)),
            pltpu.SemaphoreType.DMA((3, 6, 3)),
        ]
    )
    return pl.pallas_call(
        forward_kernel,
        name="fetch_and_retain",
        out_shape=out_shape,
        in_specs=[smem_spec(), smem_spec(), vmem_spec()] + [any_spec()] * 9,
        out_specs=[any_spec()] * 6 + [smem_spec()] + [any_spec()] * 4,
        scratch_shapes=scratch,
        compiler_params=pltpu.CompilerParams(
            collective_id=0, has_side_effects=True, vmem_limit_bytes=VMEM_LIMIT
        ),
    )(need, rate, gain, store, w_key, w_value, tokens, w_rq, w_rk, w_rv, w_q, grad)


PAIR = 2


def attention_kernel(ids_ref, gate_ref, q_ref, grad_ref, *rest):
    arrived, dq_ref, leaving = rest[:6], rest[6], rest[7:13]
    keys, values, queries, grads = rest[13:]
    factor = HEAD ** (-0.5)
    gate = jax.nn.sigmoid(gate_ref[...])
    for pair in range(PAIR):
        tokens = pl.ds(pair * BLK, BLK)
        where = []
        for slot in range(KP):
            owner = ids_ref[(pl.program_id(0) * PAIR + pair) * KP + slot] // PASS_DEV
            for channel, (kind, first, units, turn) in enumerate(CHANNELS):
                one, two, last = lines(turn)
                at = (coordinate(owner, last), coordinate(owner, two), coordinate(owner, one))
                where.append(at)
                target = values if kind else keys
                for unit in range(units):
                    row, column = unit_place(first + unit)
                    target[pair, pl.ds(slot * PLEN + row, 16), pl.ds(column, 128)] = arrived[
                        channel
                    ][at[0], at[1], at[2], unit]
        for head in range(4):
            columns = pl.ds(head * HEAD, HEAD)
            rows = pl.ds(head * BLK, BLK)
            queries[pair, rows, :] = q_ref[tokens, columns]
            grads[pair, rows, :] = (
                grad_ref[tokens, columns].astype(jnp.float32)
                * gate[:, head * HEAD : (head + 1) * HEAD]
            ).astype(jnp.bfloat16)
        expo = jnp.exp(nt(keys[pair], queries[pair]) * factor)
        probs = expo * (1.0 / jnp.sum(expo, axis=0, keepdims=True))
        probs_bf = probs.astype(jnp.bfloat16)
        grad_probs = nt(values[pair], grads[pair])
        delta = jnp.sum(probs_bf.astype(jnp.float32) * grad_probs, axis=0, keepdims=True)
        grad_scores = (probs * (grad_probs - delta) * factor).astype(jnp.bfloat16)
        key_grad = nn(grad_scores, queries[pair]).astype(jnp.bfloat16)
        value_grad = nn(probs_bf, grads[pair]).astype(jnp.bfloat16)
        query_grad = tn(grad_scores, keys[pair]).astype(jnp.bfloat16)
        for head in range(4):
            dq_ref[tokens, pl.ds(head * HEAD, HEAD)] = query_grad[head * BLK : (head + 1) * BLK]
        for slot in range(KP):
            for channel, (kind, first, units, turn) in enumerate(CHANNELS):
                at = where[slot * len(CHANNELS) + channel]
                made = value_grad if kind else key_grad
                for unit in range(units):
                    row, column = unit_place(first + unit)
                    row = row + slot * PLEN
                    leaving[channel][at[0], at[1], at[2], unit] = made[
                        row : row + 16, column : column + 128
                    ]


def attention(ids, gate, q, grad, arrived):
    bf16 = jnp.bfloat16
    length, width = q.shape
    units = [channel[2] for channel in CHANNELS]
    whole = [
        pl.BlockSpec((4, 4, 4, n, 16, 128), lambda step, ids: (0, 0, 0, 0, 0, 0)) for n in units
    ]
    rows = pl.BlockSpec((PAIR * BLK, width), lambda step, ids: (step, 0))
    return pl.pallas_call(
        attention_kernel,
        name="cross_attention",
        out_shape=[jax.ShapeDtypeStruct((length, width), bf16)]
        + [jax.ShapeDtypeStruct((4, 4, 4, n, 16, 128), bf16) for n in units],
        grid_spec=pltpu.PrefetchScalarGridSpec(
            num_scalar_prefetch=1,
            grid=(length // (PAIR * BLK),),
            in_specs=[pl.BlockSpec((1, width), lambda step, ids: (0, 0)), rows, rows] + whole,
            out_specs=[rows] + whole,
            scratch_shapes=[pltpu.VMEM((PAIR, 256, 256), bf16)] * 4,
        ),
        compiler_params=pltpu.CompilerParams(vmem_limit_bytes=VMEM_LIMIT),
    )(ids, gate, q, grad, *arrived)


def backward_kernel(
    need_ref,
    asked,
    store_any,
    w_key_any,
    w_value_any,
    dq_any,
    grq_any,
    grk_any,
    grv_any,
    w_q_any,
    w_rq_any,
    w_rk_any,
    w_rv_any,
    *rest,
):
    leaving = rest[:6]
    gt_ref, gs_ref, gw_ref = rest[6:9]
    own, third, sums, second, fewer, first_in = (
        rest[9:15],
        rest[15:21],
        rest[21:27],
        rest[27:33],
        rest[33:39],
        rest[39:45],
    )
    (
        store,
        w_key,
        w_value,
        dq,
        grq,
        grk,
        grv,
        w_q,
        w_rq,
        w_rk,
        w_rv,
        mine,
        theirs,
        passed,
        store_mine,
        store_theirs,
        store_passed,
        key_grad,
        value_grad,
        term,
        half,
        total,
        ar_first,
        ar_second,
        ar_third,
        out,
        load,
        near_send,
        near_recv,
        send,
        recv,
        ar_send,
        ar_recv,
    ) = rest[45:]
    me, core = lax.axis_index("st"), lax.axis_index("tp")
    sibling = 1 - core
    own_loads = []
    for channel, (_, _, _, turn) in enumerate(CHANNELS):
        here = coordinate(me, lines(turn)[2])
        own_loads.append(
            pltpu.make_async_copy(leaving[channel].at[here], own[channel], load.at[channel])
        )
    loads = [
        pltpu.make_async_copy(source, target, load.at[6 + at])
        for at, (source, target) in enumerate(
            (
                (dq_any, dq),
                (w_q_any, w_q),
                (grq_any, grq),
                (w_rq_any, w_rq),
                (grk_any, grk),
                (w_rk_any, w_rk),
                (grv_any, grv),
                (w_rv_any, w_rv),
                (store_any, store),
                (w_key_any, w_key),
                (w_value_any, w_value),
            )
        )
    ]
    line_barrier(me, sibling)

    def remote(stage, channel, step, dim, source, target):
        return pltpu.make_async_remote_copy(
            src_ref=source,
            dst_ref=target,
            send_sem=send.at[stage, channel, step - 1],
            recv_sem=recv.at[stage, channel, step - 1],
            device_id={"st": peer_of(me, dim, step)},
            device_id_type=MESH,
        )

    def third_stage(channels):
        copies = {}
        for channel in channels:
            last = lines(CHANNELS[channel][3])[2]
            at = coordinate(me, last)
            for step in STEPS:
                copies[channel, step] = remote(
                    0,
                    channel,
                    step,
                    last,
                    leaving[channel].at[lax.rem(at + step, 4)],
                    third[channel].at[step - 1],
                )
                copies[channel, step].start()
        return copies

    def second_stage(channels, before):
        copies = {}
        for channel in channels:
            one, two, last = lines(CHANNELS[channel][3])
            here = coordinate(me, last)
            own_loads[channel].wait()
            for step in STEPS:
                before[channel, step].wait()

            @pl.loop(0, 16)
            def _(at):
                beside, along = at // 4, lax.rem(at, 4)
                owner = along * STRIDES[one] + beside * STRIDES[two] + here * STRIDES[last]
                names = [need_ref[0, 0, owner]] + [
                    asked[last * 3 + step - 1, 0, owner] for step in STEPS
                ]
                rows = [own[channel][beside, along].astype(jnp.float32)] + [
                    third[channel][step - 1, beside, along].astype(jnp.float32) for step in STEPS
                ]
                for passage in range(PASS_DEV):
                    held = jnp.zeros_like(rows[0])
                    for name, row in zip(names, rows):
                        held = held + row * jnp.where(name == passage, 1.0, 0.0)
                    sums[channel][beside, along, passage] = held.astype(jnp.bfloat16)

            at = coordinate(me, two)
            for step in STEPS:
                copies[channel, step] = remote(
                    1,
                    channel,
                    step,
                    two,
                    sums[channel].at[lax.rem(at + step, 4)],
                    second[channel].at[step - 1],
                )
                copies[channel, step].start()
        return copies

    def first_stage(channels, before):
        copies = {}
        for channel in channels:
            one, two, _ = lines(CHANNELS[channel][3])
            for step in STEPS:
                before[channel, step].wait()
            here = coordinate(me, two)
            held = sums[channel][here].astype(jnp.float32)
            for step in STEPS:
                held = held + second[channel][step - 1].astype(jnp.float32)
            fewer[channel][...] = held.astype(jnp.bfloat16)
            at = coordinate(me, one)
            for step in STEPS:
                copies[channel, step] = remote(
                    2,
                    channel,
                    step,
                    one,
                    fewer[channel].at[lax.rem(at + step, 4)],
                    first_in[channel].at[step - 1],
                )
                copies[channel, step].start()
        return copies

    def passage_sums(channels, before, target):
        for channel in channels:
            _, first, units, turn = CHANNELS[channel]
            for step in STEPS:
                before[channel, step].wait()
            held = fewer[channel][coordinate(me, turn)].astype(jnp.float32)
            for step in STEPS:
                held = held + first_in[channel][step - 1].astype(jnp.float32)
            held = held.astype(jnp.bfloat16)
            for passage in range(PASS_DEV):
                for unit in range(units):
                    row, column = unit_place(first + unit)
                    target[pl.ds(passage * PLEN + row, 16), pl.ds(column, 128)] = held[
                        passage, unit
                    ]

    def near(at, source, target):
        return pltpu.make_async_remote_copy(
            src_ref=source,
            dst_ref=target,
            send_sem=near_send.at[at],
            recv_sem=near_recv.at[at],
            device_id={"tp": sibling},
            device_id_type=MESH,
        )

    length = dq.shape[0]
    part = length // 2

    def rows_of(left):
        return jnp.concatenate(
            [left[aligned(sibling * part, part), :], left[aligned(core * part, part), :]], axis=0
        )

    def token_grads(start, stop):
        @pl.loop(start, stop)
        def _(tile):
            columns = aligned(tile * 256, 256, 256)
            made = nt(rows_of(dq), w_q[columns, :])
            made = made + nt(rows_of(grq), w_rq[columns, :])
            made = made + nt(rows_of(grk), w_rk[columns, :])
            made = made + nt(rows_of(grv), w_rv[columns, :])
            theirs[tile] = made[:part].astype(jnp.bfloat16)
            mine[tile] = made[part:]
            near(tile, theirs.at[tile], passed.at[tile]).start()

    def token_ends(start, stop):
        @pl.loop(start, stop)
        def _(tile):
            near(tile, theirs.at[tile], passed.at[tile]).wait()
            columns = aligned(tile * 256, 256, 256)
            gt_ref[:, columns] = (mine[tile] + passed[tile].astype(jnp.float32)).astype(
                jnp.bfloat16
            )

    keys = third_stage(KEY_CHANNELS)
    values = third_stage(VALUE_CHANNELS)
    for one in loads + own_loads:
        one.start()
    for one in loads[:8]:
        one.wait()
    token_grads(0, 3)
    keys = second_stage(KEY_CHANNELS, keys)
    token_grads(3, 5)
    values = second_stage(VALUE_CHANNELS, values)
    token_grads(5, 6)
    keys = first_stage(KEY_CHANNELS, keys)
    token_grads(6, 8)
    values = first_stage(VALUE_CHANNELS, values)
    for one in loads[8:]:
        one.wait()
    passage_sums(KEY_CHANNELS, keys, key_grad)
    term[...] = tn(store[...], key_grad[...])
    half[...] = term[...].astype(jnp.bfloat16)

    def ar_copy(stage, place, step, dim, source, target):
        return pltpu.make_async_remote_copy(
            src_ref=source,
            dst_ref=target,
            send_sem=ar_send.at[stage, place, step - 1],
            recv_sem=ar_recv.at[stage, place, step - 1],
            device_id={"st": peer_of(me, dim, step)},
            device_id_type=MESH,
        )

    started = []
    for place, (start, size) in enumerate(PARTS):
        at = coordinate(me, place)
        quarter = size // 4
        for step in STEPS:
            there = lax.rem(at + step, 4)
            one = ar_copy(
                0,
                place,
                step,
                place,
                half.at[aligned(start + there * quarter, quarter)],
                ar_first.at[step - 1, pl.ds(start // 4, quarter)],
            )
            one.start()
            started.append(one)
    passage_sums(VALUE_CHANNELS, values, value_grad)
    store_rows = 2 * PLEN
    made = nt(
        jnp.concatenate(
            [
                key_grad[aligned(sibling * store_rows, store_rows), :],
                key_grad[aligned(core * store_rows, store_rows), :],
            ],
            axis=0,
        ),
        w_key[...],
    ) + nt(
        jnp.concatenate(
            [
                value_grad[aligned(sibling * store_rows, store_rows), :],
                value_grad[aligned(core * store_rows, store_rows), :],
            ],
            axis=0,
        ),
        w_value[...],
    )
    store_theirs[...] = made[:store_rows].astype(jnp.bfloat16)
    store_mine[...] = made[store_rows:]
    store_near = near(8, store_theirs, store_passed)
    store_near.start()
    stage = []
    for place, (start, size) in enumerate(PARTS):
        other = (place + 1) % 3
        at, beside = coordinate(me, place), coordinate(me, other)
        quarter, small = size // 4, size // 16
        base = start + at * quarter
        for step in STEPS:
            started[place * 3 + step - 1].wait()
        held = term[aligned(base, quarter), :]
        for step in STEPS:
            held = held + ar_first[step - 1, pl.ds(start // 4, quarter), :].astype(jnp.float32)
        total[pl.ds(start // 4, quarter), :] = held
        half[aligned(base, quarter), :] = held.astype(jnp.bfloat16)
        for step in STEPS:
            there = lax.rem(beside + step, 4)
            one = ar_copy(
                1,
                place,
                step,
                other,
                half.at[aligned(base + there * small, small)],
                ar_second.at[step - 1, pl.ds(start // 16, small)],
            )
            one.start()
            stage.append(one)
    token_ends(0, 4)
    started, stage = stage, []
    for place, (start, size) in enumerate(PARTS):
        _, other, last = lines(place)
        at, beside = coordinate(me, place), coordinate(me, other)
        quarter, small = size // 4, size // 16
        base = start + at * quarter + beside * small
        for step in STEPS:
            started[place * 3 + step - 1].wait()
        held = total[aligned(start // 4 + beside * small, small), :]
        for step in STEPS:
            held = held + ar_second[step - 1, pl.ds(start // 16, small), :].astype(jnp.float32)
        half[aligned(base, small), :] = held.astype(jnp.bfloat16)
        for step in STEPS:
            one = ar_copy(
                2,
                place,
                step,
                last,
                half.at[aligned(base, small)],
                ar_third.at[step - 1, pl.ds(start // 16, small)],
            )
            one.start()
            stage.append(one)
    token_ends(4, 8)
    started, stage = stage, []
    for place, (start, size) in enumerate(PARTS):
        other = (place + 1) % 3
        at, beside = coordinate(me, place), coordinate(me, other)
        quarter, small = size // 4, size // 16
        base = start + at * quarter + beside * small
        for step in STEPS:
            started[place * 3 + step - 1].wait()
        rows = pl.ds(start // 16, small)
        held = half[aligned(base, small), :].astype(jnp.float32) + ar_third[1, rows, :].astype(
            jnp.float32
        )
        held = held + (
            ar_third[0, rows, :].astype(jnp.float32) + ar_third[2, rows, :].astype(jnp.float32)
        )
        out[aligned(base, small), :] = held.astype(jnp.bfloat16)
        for step in STEPS:
            here = out.at[aligned(base, small)]
            one = ar_copy(3, place, step, other, here, here)
            one.start()
            stage.append(one)
    store_near.wait()
    gs_ref[...] = (store_mine[...] + store_passed[...].astype(jnp.float32)).astype(jnp.bfloat16)
    started, stage = stage, []
    for place, (start, size) in enumerate(PARTS):
        at = coordinate(me, place)
        quarter = size // 4
        base = start + at * quarter
        for step in STEPS:
            started[place * 3 + step - 1].wait()
        for step in STEPS:
            here = out.at[aligned(base, quarter)]
            one = ar_copy(4, place, step, place, here, here)
            one.start()
            stage.append(one)
    for one in stage:
        one.wait()
    gw_ref[...] = out[...].astype(jnp.float32)


def backward(
    need, asked, store, w_key, w_value, dq, grq, grk, grv, w_q, w_rq, w_rk, w_rv, leaving
):
    bf16, f32 = jnp.bfloat16, jnp.float32
    length, width = dq.shape[0], store.shape[1]
    units = [channel[2] for channel in CHANNELS]
    kv_width = w_key.shape[1]
    tiles = width // 256
    scratch = (
        [pltpu.VMEM((4, 4, n, 16, 128), bf16) for n in units]
        + [pltpu.VMEM((3, 4, 4, n, 16, 128), bf16) for n in units]
        + [pltpu.VMEM((4, 4, 4, n, 16, 128), bf16) for n in units]
        + [pltpu.VMEM((3, 4, 4, n, 16, 128), bf16) for n in units]
        + [pltpu.VMEM((4, 4, n, 16, 128), bf16) for n in units]
        + [pltpu.VMEM((3, 4, n, 16, 128), bf16) for n in units]
        + [
            pltpu.VMEM(array.shape, array.dtype)
            for array in (store, w_key, w_value, dq, grq, grk, grv, w_q, w_rq, w_rk, w_rv)
        ]
        + [
            pltpu.VMEM((tiles, length // 2, 256), f32),
            pltpu.VMEM((tiles, length // 2, 256), bf16),
            pltpu.VMEM((tiles, length // 2, 256), bf16),
            pltpu.VMEM((2 * PLEN, width), f32),
            pltpu.VMEM((2 * PLEN, width), bf16),
            pltpu.VMEM((2 * PLEN, width), bf16),
            pltpu.VMEM((PASS_DEV * PLEN, kv_width), bf16),
            pltpu.VMEM((PASS_DEV * PLEN, kv_width), bf16),
            pltpu.VMEM((width, kv_width), f32),
            pltpu.VMEM((width, kv_width), bf16),
            pltpu.VMEM((width // 4, kv_width), f32),
            pltpu.VMEM((3, width // 4, kv_width), bf16),
            pltpu.VMEM((3, width // 16, kv_width), bf16),
            pltpu.VMEM((3, width // 16, kv_width), bf16),
            pltpu.VMEM((width, kv_width), bf16),
            pltpu.SemaphoreType.DMA((17,)),
            pltpu.SemaphoreType.DMA((9,)),
            pltpu.SemaphoreType.DMA((9,)),
            pltpu.SemaphoreType.DMA((3, 6, 3)),
            pltpu.SemaphoreType.DMA((3, 6, 3)),
            pltpu.SemaphoreType.DMA((5, 3, 3)),
            pltpu.SemaphoreType.DMA((5, 3, 3)),
        ]
    )
    return pl.pallas_call(
        backward_kernel,
        name="return_and_reduce",
        out_shape=[
            jax.ShapeDtypeStruct((length // 2, width), bf16),
            jax.ShapeDtypeStruct((2 * PLEN, width), bf16),
            jax.ShapeDtypeStruct((width, kv_width), f32),
        ],
        in_specs=[smem_spec(), smem_spec()] + [any_spec()] * 17,
        out_specs=[vmem_spec()] * 3,
        scratch_shapes=scratch,
        compiler_params=pltpu.CompilerParams(
            collective_id=1, has_side_effects=True, vmem_limit_bytes=VMEM_LIMIT
        ),
    )(need, asked, store, w_key, w_value, dq, grq, grk, grv, w_q, w_rq, w_rk, w_rv, *leaving)


def per_device(
    tokens,
    store,
    passage_ids,
    w_query,
    w_key,
    w_value,
    w_ret_query,
    w_ret_key,
    w_ret_value,
    ret_rate,
    ret_gain,
    gate_logit,
    out_grad,
):
    width = store.shape[2]
    ids = passage_ids.reshape(-1)
    owners = jnp.arange(128, dtype=jnp.int32)
    need = jnp.sum(
        jnp.where(owners[:, None] == (ids // PASS_DEV)[None, :], (ids % PASS_DEV)[None, :], 0),
        axis=1,
    ).reshape(1, 1, 128)
    store_rows = store.reshape(-1, width)
    made = forward(
        need,
        ret_rate,
        ret_gain.reshape(1, -1),
        store_rows,
        w_key,
        w_value,
        tokens,
        w_ret_query,
        w_ret_key,
        w_ret_value,
        w_query,
        out_grad,
    )
    arrived, (asked, q, grq, grk, grv) = made[:6], made[6:]
    dq, *leaving = attention(ids, gate_logit.reshape(1, -1), q, out_grad, arrived)
    grad_tokens, grad_store, grad_key_weight = backward(
        need,
        asked,
        store_rows,
        w_key,
        w_value,
        dq,
        grq,
        grk,
        grv,
        w_query,
        w_ret_query,
        w_ret_key,
        w_ret_value,
        leaving,
    )
    return (grad_tokens, grad_store.reshape(-1, PLEN, width), grad_key_weight)


def solution(mesh):
    return jax.shard_map(
        per_device,
        mesh=mesh,
        in_specs=(
            P("st", None),
            P("st", None, None),
            P("st", None),
            P(None, "tp"),
            P(None, "tp"),
            P(None, "tp"),
            P(None, "tp"),
            P(None, "tp"),
            P(None, "tp"),
            P("tp"),
            P("tp"),
            P("tp"),
            P("st", "tp"),
        ),
        out_specs=(P(("st", "tp"), None), P(("st", "tp"), None, None), P(None, "tp")),
        check_vma=False,
    )
```

```python
import functools

import jax
import jax.numpy as jnp
from jax import lax
from jax.experimental import pallas as pl
from jax.experimental.pallas import tpu as pltpu
from jax.sharding import PartitionSpec as P

MESH = pl.DeviceIdType.MESH
HEAD = 256
BLK = 64
KP = 4
PLEN = 64
PASS_DEV = 4
OWNERS = 64
RET_KEY = 128
EPSILON = 1.0
VMEM_LIMIT = 60 * 1024 * 1024

CHANNELS = (
    (0, 0, 3, 0),
    (0, 3, 3, 1),
    (0, 6, 2, 2),
    (1, 0, 2, 0),
    (1, 2, 3, 1),
    (1, 5, 3, 2),
)
KEY_CHANNELS = (0, 1, 2)
VALUE_CHANNELS = (3, 4, 5)
STEPS = (1, 2, 3)
PARTS = ((0, 768), (768, 768), (1536, 512))


def nn(left, right):
    return jnp.dot(left, right, preferred_element_type=jnp.float32)


def nt(left, right):
    return lax.dot_general(
        left, right, (((1,), (1,)), ((), ())), preferred_element_type=jnp.float32
    )


def tn(left, right):
    return lax.dot_general(
        left, right, (((0,), (0,)), ((), ())), preferred_element_type=jnp.float32
    )


def stride(dim):
    return (9 * dim * dim - 3 * dim + 2) // 2


def coordinate(index, dim):
    return lax.rem(index // stride(dim), 4)


def peer_of(me, dim, step):
    at = coordinate(me, dim)
    return me + (lax.rem(at + step, 4) - at) * stride(dim)


def lines(turn):
    first = turn + lax.axis_index("tp")
    return lax.rem(first, 3), lax.rem(first + 1, 3), lax.rem(first + 2, 3)


def line_barrier(me, sibling=None):
    barrier = pltpu.get_barrier_semaphore()
    for dim in range(3):
        for step in STEPS:
            pl.semaphore_signal(
                barrier, inc=1, device_id={"st": peer_of(me, dim, step)}, device_id_type=MESH
            )
    if sibling is None:
        pl.semaphore_wait(barrier, 9)
    else:
        pl.semaphore_signal(barrier, inc=1, device_id={"tp": sibling}, device_id_type=MESH)
        pl.semaphore_wait(barrier, 10)


def aligned(start, size, by=16):
    return pl.ds(pl.multiple_of(start, by), size)


def unit_place(unit):
    return (unit // 2) * 16, (unit % 2) * 128


def forward_kernel(
    need_ref,
    rate_ref,
    gain_ref,
    store_any,
    w_key_any,
    w_value_any,
    tokens_any,
    w_rq_any,
    w_rk_any,
    w_rv_any,
    w_q_any,
    grad_any,
    *rest,
):
    arrived = rest[:6]
    asked, q_any, grq_any, grk_any, grv_any = rest[6:11]
    table, outgoing, own = rest[11:17], rest[17:23], rest[23:29]
    (
        store,
        w_key,
        w_value,
        tokens,
        w_rq,
        w_rk,
        w_rv,
        w_q,
        grad,
        rq,
        rk,
        rv,
        q,
        grq,
        grk,
        grv,
        damp,
        weights,
        grad_weights,
        grad_y,
        load,
        leave,
        id_send,
        id_recv,
        send,
        recv,
    ) = rest[29:]
    me = lax.axis_index("st")
    loads = [
        pltpu.make_async_copy(source, target, load.at[at])
        for at, (source, target) in enumerate(
            (
                (store_any, store),
                (w_key_any, w_key),
                (w_value_any, w_value),
                (tokens_any, tokens),
                (w_rq_any, w_rq),
                (w_rk_any, w_rk),
                (w_rv_any, w_rv),
                (grad_any, grad),
                (w_q_any, w_q),
            )
        )
    ]
    for one in loads:
        one.start()
    line_barrier(me)
    names = []
    for dim in range(3):
        for step in STEPS:
            at = dim * 3 + step - 1
            one = pltpu.make_async_remote_copy(
                src_ref=need_ref.at[0],
                dst_ref=asked.at[at],
                send_sem=id_send.at[at],
                recv_sem=id_recv.at[at],
                device_id={"st": peer_of(me, dim, step)},
                device_id_type=MESH,
            )
            one.start()
            names.append(one)

    def remote(stage, channel, step, dim, source, target):
        return pltpu.make_async_remote_copy(
            src_ref=source,
            dst_ref=target,
            send_sem=send.at[stage, channel, step - 1],
            recv_sem=recv.at[stage, channel, step - 1],
            device_id={"st": peer_of(me, dim, step)},
            device_id_type=MESH,
        )

    def own_rows(kind, weight):
        made = nn(store[...], weight[...]).astype(jnp.bfloat16)
        for channel, (which, first, units, turn) in enumerate(CHANNELS):
            if which != kind:
                continue
            one, two, _ = lines(turn)
            at, beside = coordinate(me, one), coordinate(me, two)
            for passage in range(PASS_DEV):
                for unit in range(units):
                    row, column = unit_place(first + unit)
                    row = row + passage * PLEN
                    table[channel][beside, at, passage, unit] = made[
                        row : row + 16, column : column + 128
                    ]

    def first_stage(channels):
        copies = {}
        for channel in channels:
            one, two, _ = lines(CHANNELS[channel][3])
            at, beside = coordinate(me, one), coordinate(me, two)
            here = table[channel].at[beside, at]
            for step in STEPS:
                copies[channel, step] = remote(0, channel, step, one, here, here)
                copies[channel, step].start()
        return copies

    def second_stage(channels, before):
        copies = {}
        for channel in channels:
            _, two, _ = lines(CHANNELS[channel][3])
            for step in STEPS:
                before[channel, step].wait()
            here = table[channel].at[coordinate(me, two)]
            for step in STEPS:
                copies[channel, step] = remote(1, channel, step, two, here, here)
                copies[channel, step].start()
        return copies

    def third_stage(channels, before):
        copies = {}
        for channel in channels:
            one, two, last = lines(CHANNELS[channel][3])
            here = coordinate(me, last)
            for step in STEPS:
                before[channel, step].wait()

            @pl.loop(0, 16, unroll=4)
            def _(at):
                beside, along = at // 4, lax.rem(at, 4)
                owner = along * stride(one) + beside * stride(two) + here * stride(last)
                own[channel][beside, along] = table[channel][beside, along, need_ref[0, 0, owner]]
                for step in STEPS:
                    row = last * 3 + (4 - step) - 1
                    outgoing[channel][step - 1, beside, along] = table[channel][
                        beside, along, asked[row, 0, owner]
                    ]

            for step in STEPS:
                copies[channel, step] = remote(
                    2,
                    channel,
                    step,
                    last,
                    outgoing[channel].at[step - 1],
                    arrived[channel].at[here],
                )
                copies[channel, step].start()
            copies[channel, 0] = pltpu.make_async_copy(
                own[channel], arrived[channel].at[here], leave.at[channel]
            )
            copies[channel, 0].start()
        return copies

    def project(weight, target):
        @pl.loop(0, weight.shape[1] // 256)
        def _(tile):
            columns = aligned(tile * 256, 256, 256)
            target[:, columns] = nn(tokens[...], weight[:, columns]).astype(jnp.bfloat16)

    def retention(start, stop):
        @pl.loop(start, stop)
        def _(head):
            rate = rate_ref[head]
            narrow = aligned(head * RET_KEY, RET_KEY, 128)
            wide = aligned(head * HEAD, HEAD, 256)
            rows = lax.broadcasted_iota(jnp.int32, (256, 256), 0)
            columns = lax.broadcasted_iota(jnp.int32, (256, 256), 1)
            for apart in range(4):
                distance = (rows - columns + 256 * apart).astype(jnp.float32)
                damp[apart] = jnp.where(
                    distance >= 0.0, jnp.exp(-rate * jnp.maximum(distance, 0.0)), 0.0
                ) * RET_KEY ** (-0.5)
            for i in range(4):
                block = pl.ds(i * 256, 256)
                upto = (i + 1) * 256
                for j in range(i + 1):
                    raw = nt(rq[block, narrow], rk[pl.ds(j * 256, 256), narrow])
                    weights[block, pl.ds(j * 256, 256)] = (raw * damp[i - j]).astype(jnp.bfloat16)
                y = nn(weights[block, pl.ds(0, upto)], rv[pl.ds(0, upto), wide])
                inverse = lax.rsqrt(jnp.mean(y * y, axis=1, keepdims=True) + EPSILON)
                scaled = grad[block, wide].astype(jnp.float32) * gain_ref[:, wide]
                inner = jnp.mean(scaled * y, axis=1, keepdims=True)
                grad_y[block, :] = (
                    inverse * scaled - (inverse * inverse * inverse * inner) * y
                ).astype(jnp.bfloat16)
                for j in range(i + 1):
                    raw = nt(grad_y[block, :], rv[pl.ds(j * 256, 256), wide])
                    grad_weights[block, pl.ds(j * 256, 256)] = (raw * damp[i - j]).astype(
                        jnp.bfloat16
                    )
                grq[block, narrow] = nn(
                    grad_weights[block, pl.ds(0, upto)], rk[pl.ds(0, upto), narrow]
                ).astype(jnp.bfloat16)
            for j in range(4):
                block = pl.ds(j * 256, 256)
                after = pl.ds(j * 256, 1024 - j * 256)
                grk[block, narrow] = tn(grad_weights[after, block], rq[after, narrow]).astype(
                    jnp.bfloat16
                )
                grv[block, wide] = tn(weights[after, block], grad_y[after, :]).astype(jnp.bfloat16)

    loads[0].wait()
    loads[1].wait()
    own_rows(0, w_key)
    keys = first_stage(KEY_CHANNELS)
    loads[2].wait()
    own_rows(1, w_value)
    values = first_stage(VALUE_CHANNELS)
    for one in names:
        one.wait()
    loads[3].wait()
    loads[4].wait()
    project(w_rq, rq)
    keys = second_stage(KEY_CHANNELS, keys)
    values = second_stage(VALUE_CHANNELS, values)
    loads[5].wait()
    project(w_rk, rk)
    loads[6].wait()
    project(w_rv, rv)
    loads[7].wait()
    retention(0, 1)
    keys = third_stage(KEY_CHANNELS, keys)
    retention(1, 2)
    values = third_stage(VALUE_CHANNELS, values)
    loads[8].wait()
    project(w_q, q)
    ends = [pltpu.make_async_copy(q, q_any, leave.at[6])]
    ends[0].start()
    retention(2, 4)
    for at, (source, target) in enumerate(((grq, grq_any), (grk, grk_any), (grv, grv_any))):
        one = pltpu.make_async_copy(source, target, leave.at[7 + at])
        one.start()
        ends.append(one)
    for one in list(keys.values()) + list(values.values()) + ends:
        one.wait()


def any_spec():
    return pl.BlockSpec(memory_space=pl.ANY)


def vmem_spec():
    return pl.BlockSpec(memory_space=pltpu.VMEM)


def smem_spec():
    return pl.BlockSpec(memory_space=pltpu.SMEM)


def forward(need, rate, gain, store, w_key, w_value, tokens, w_rq, w_rk, w_rv, w_q, grad):
    bf16, f32 = jnp.bfloat16, jnp.float32
    length, width = tokens.shape
    units = [channel[2] for channel in CHANNELS]
    out_shape = (
        [jax.ShapeDtypeStruct((4, 4, 4, n, 16, 128), bf16) for n in units]
        + [jax.ShapeDtypeStruct((9, 1, 128), jnp.int32)]
        + [
            jax.ShapeDtypeStruct((length, n), bf16)
            for n in (w_q.shape[1], w_rq.shape[1], w_rk.shape[1], w_rv.shape[1])
        ]
    )
    scratch = (
        [pltpu.VMEM((4, 4, 4, n, 16, 128), bf16) for n in units]
        + [pltpu.VMEM((3, 4, 4, n, 16, 128), bf16) for n in units]
        + [pltpu.VMEM((4, 4, n, 16, 128), bf16) for n in units]
        + [
            pltpu.VMEM(array.shape, array.dtype)
            for array in (store, w_key, w_value, tokens, w_rq, w_rk, w_rv, w_q, grad)
        ]
        + [
            pltpu.VMEM((length, n), bf16)
            for n in (w_rq.shape[1], w_rk.shape[1], w_rv.shape[1], w_q.shape[1])
        ]
        + [pltpu.VMEM((length, n), bf16) for n in (w_rq.shape[1], w_rk.shape[1], w_rv.shape[1])]
        + [
            pltpu.VMEM((4, 256, 256), f32),
            pltpu.VMEM((length, length), bf16),
            pltpu.VMEM((length, length), bf16),
            pltpu.VMEM((length, HEAD), bf16),
            pltpu.SemaphoreType.DMA((9,)),
            pltpu.SemaphoreType.DMA((10,)),
            pltpu.SemaphoreType.DMA((9,)),
            pltpu.SemaphoreType.DMA((9,)),
            pltpu.SemaphoreType.DMA((3, 6, 3)),
            pltpu.SemaphoreType.DMA((3, 6, 3)),
        ]
    )
    return pl.pallas_call(
        forward_kernel,
        name="fetch_and_retain",
        out_shape=out_shape,
        in_specs=[smem_spec(), smem_spec(), vmem_spec()] + [any_spec()] * 9,
        out_specs=[any_spec()] * 6 + [smem_spec()] + [any_spec()] * 4,
        scratch_shapes=scratch,
        compiler_params=pltpu.CompilerParams(
            collective_id=0, has_side_effects=True, vmem_limit_bytes=VMEM_LIMIT
        ),
    )(need, rate, gain, store, w_key, w_value, tokens, w_rq, w_rk, w_rv, w_q, grad)


PAIR = 4


def attention_kernel(ids_ref, gate_ref, q_ref, grad_ref, *rest):
    arrived, dq_ref, leaving = rest[:6], rest[6], rest[7:13]
    keys, values, queries, grads = rest[13:]
    factor = HEAD ** (-0.5)
    gate = jax.nn.sigmoid(gate_ref[...])
    core = lax.axis_index("tp")
    where = {}
    for pair in range(PAIR):
        tokens = pl.ds(pair * BLK, BLK)
        for slot in range(KP):
            owner = ids_ref[(pl.program_id(0) * PAIR + pair) * KP + slot] // PASS_DEV
            for turn in range(3):
                shift = 2 * lax.rem(turn + core, 3)
                where[pair, slot, turn] = (owner >> shift) | ((owner << (6 - shift)) & 63)
            for channel, (kind, first, units, turn) in enumerate(CHANNELS):
                target = values if kind else keys
                for unit in range(units):
                    row, column = unit_place(first + unit)
                    target[pair, pl.ds(slot * PLEN + row, 16), pl.ds(column, 128)] = arrived[
                        channel
                    ][where[pair, slot, turn], unit]
        for head in range(4):
            columns = pl.ds(head * HEAD, HEAD)
            rows = pl.ds(head * BLK, BLK)
            queries[pair, rows, :] = q_ref[tokens, columns]
            grads[pair, rows, :] = (
                grad_ref[tokens, columns].astype(jnp.float32)
                * gate[:, head * HEAD : (head + 1) * HEAD]
            ).astype(jnp.bfloat16)
    pairs = range(PAIR)
    expo = [jnp.exp(nt(keys[pair], queries[pair]) * factor) for pair in pairs]
    grad_probs = [nt(values[pair], grads[pair]) for pair in pairs]
    probs = [one * (1.0 / jnp.sum(one, axis=0, keepdims=True)) for one in expo]
    probs_bf = [one.astype(jnp.bfloat16) for one in probs]
    delta = [
        jnp.sum(one.astype(jnp.float32) * other, axis=0, keepdims=True)
        for one, other in zip(probs_bf, grad_probs)
    ]
    grad_scores = [
        (one * (other - third) * factor).astype(jnp.bfloat16)
        for one, other, third in zip(probs, grad_probs, delta)
    ]
    for pair in pairs:
        tokens = pl.ds(pair * BLK, BLK)
        key_grad = nn(grad_scores[pair], queries[pair]).astype(jnp.bfloat16)
        value_grad = nn(probs_bf[pair], grads[pair]).astype(jnp.bfloat16)
        query_grad = tn(grad_scores[pair], keys[pair]).astype(jnp.bfloat16)
        for head in range(4):
            dq_ref[tokens, pl.ds(head * HEAD, HEAD)] = query_grad[head * BLK : (head + 1) * BLK]
        for slot in range(KP):
            for channel, (kind, first, units, turn) in enumerate(CHANNELS):
                made = value_grad if kind else key_grad
                for unit in range(units):
                    row, column = unit_place(first + unit)
                    row = row + slot * PLEN
                    leaving[channel][where[pair, slot, turn], unit] = made[
                        row : row + 16, column : column + 128
                    ]


def attention(ids, gate, q, grad, arrived):
    bf16 = jnp.bfloat16
    length, width = q.shape
    units = [channel[2] for channel in CHANNELS]
    whole = [pl.BlockSpec((OWNERS, n, 16, 128), lambda step, ids: (0, 0, 0, 0)) for n in units]
    rows = pl.BlockSpec((PAIR * BLK, width), lambda step, ids: (step, 0))
    dq, *leaving = pl.pallas_call(
        attention_kernel,
        name="cross_attention",
        out_shape=[jax.ShapeDtypeStruct((length, width), bf16)]
        + [jax.ShapeDtypeStruct((OWNERS, n, 16, 128), bf16) for n in units],
        grid_spec=pltpu.PrefetchScalarGridSpec(
            num_scalar_prefetch=1,
            grid=(length // (PAIR * BLK),),
            in_specs=[pl.BlockSpec((1, width), lambda step, ids: (0, 0)), rows, rows] + whole,
            out_specs=[rows] + whole,
            scratch_shapes=[pltpu.VMEM((PAIR, 256, 256), bf16)] * 4,
        ),
        compiler_params=pltpu.CompilerParams(vmem_limit_bytes=VMEM_LIMIT),
    )(ids, gate, q, grad, *[one.reshape(OWNERS, -1, 16, 128) for one in arrived])
    return dq, [one.reshape(4, 4, 4, -1, 16, 128) for one in leaving]


def backward_kernel(
    need_ref,
    asked,
    store_any,
    w_key_any,
    w_value_any,
    dq_any,
    grq_any,
    grk_any,
    grv_any,
    w_q_any,
    w_rq_any,
    w_rk_any,
    w_rv_any,
    *rest,
):
    leaving = rest[:6]
    gt_any, gs_any, out = rest[6:9]
    own, third, sums, second, fewer, first_in = (
        rest[9:15],
        rest[15:21],
        rest[21:27],
        rest[27:33],
        rest[33:39],
        rest[39:45],
    )
    (
        store,
        w_key,
        w_value,
        dq,
        grq,
        grk,
        grv,
        w_q,
        w_rq,
        w_rk,
        w_rv,
        mine,
        theirs,
        passed,
        store_mine,
        store_theirs,
        store_passed,
        key_grad,
        value_grad,
        term,
        half,
        total,
        ar_first,
        ar_second,
        ar_third,
        gt,
        gs,
        flipped,
        load,
        near_send,
        near_recv,
        send,
        recv,
        ar_send,
        ar_recv,
    ) = rest[45:]
    me, core = lax.axis_index("st"), lax.axis_index("tp")
    sibling = 1 - core
    own_loads = []
    for channel, (_, _, _, turn) in enumerate(CHANNELS):
        here = coordinate(me, lines(turn)[2])
        own_loads.append(
            pltpu.make_async_copy(leaving[channel].at[here], own[channel], load.at[channel])
        )
    loads = [
        pltpu.make_async_copy(source, target, load.at[6 + at])
        for at, (source, target) in enumerate(
            (
                (dq_any, dq),
                (w_q_any, w_q),
                (grq_any, grq),
                (w_rq_any, w_rq),
                (grk_any, grk),
                (w_rk_any, w_rk),
                (grv_any, grv),
                (w_rv_any, w_rv),
                (store_any, store),
                (w_key_any, w_key),
                (w_value_any, w_value),
            )
        )
    ]
    line_barrier(me, sibling)

    def remote(stage, channel, step, dim, source, target, half=0):
        return pltpu.make_async_remote_copy(
            src_ref=source,
            dst_ref=target,
            send_sem=send.at[stage, channel, step - 1, half],
            recv_sem=recv.at[stage, channel, step - 1, half],
            device_id={"st": peer_of(me, dim, step)},
            device_id_type=MESH,
        )

    def third_stage(channels, halves):
        copies = {}
        for channel in channels:
            last = lines(CHANNELS[channel][3])[2]
            at = coordinate(me, last)
            for half, rows in halves:
                for step in STEPS:
                    one = remote(
                        0,
                        channel,
                        step,
                        last,
                        leaving[channel].at[lax.rem(at + step, 4), rows],
                        third[channel].at[step - 1, rows],
                        half,
                    )
                    one.start()
                    copies[channel, half, step] = one
        return copies

    def add_readers(channels, before, start, stop):
        for channel in channels:
            one, two, last = lines(CHANNELS[channel][3])
            here = coordinate(me, last)
            for (which, _, _), copy in before.items():
                if which == channel:
                    copy.wait()

            @pl.loop(start * 4, stop * 4, unroll=4)
            def _(at):
                beside, along = at // 4, lax.rem(at, 4)
                owner = along * stride(one) + beside * stride(two) + here * stride(last)
                names = [need_ref[0, 0, owner]] + [
                    asked[last * 3 + step - 1, 0, owner] for step in STEPS
                ]
                rows = [own[channel][beside, along].astype(jnp.float32)] + [
                    third[channel][step - 1, beside, along].astype(jnp.float32) for step in STEPS
                ]
                for passage in range(PASS_DEV):
                    terms = [
                        row * jnp.where(name == passage, 1.0, 0.0) for name, row in zip(names, rows)
                    ]
                    held = (terms[0] + terms[1]) + (terms[2] + terms[3])
                    sums[channel][beside, along, passage] = held.astype(jnp.bfloat16)

    def second_stage(channels, halves):
        copies = {}
        for channel in channels:
            _, two, _ = lines(CHANNELS[channel][3])
            at = coordinate(me, two)
            for half, rows in halves:
                for step in STEPS:
                    one = remote(
                        1,
                        channel,
                        step,
                        two,
                        sums[channel].at[lax.rem(at + step, 4), rows],
                        second[channel].at[step - 1, rows],
                        half,
                    )
                    one.start()
                    copies[channel, half, step] = one
        return copies

    def first_stage(channels, before):
        copies = {}
        for channel in channels:
            one, two, _ = lines(CHANNELS[channel][3])
            for (which, _, _), copy in before.items():
                if which == channel:
                    copy.wait()
            here = coordinate(me, two)
            held = sums[channel][here].astype(jnp.float32)
            for step in STEPS:
                held = held + second[channel][step - 1].astype(jnp.float32)
            fewer[channel][...] = held.astype(jnp.bfloat16)
            at = coordinate(me, one)
            for step in STEPS:
                copies[channel, step] = remote(
                    2,
                    channel,
                    step,
                    one,
                    fewer[channel].at[lax.rem(at + step, 4)],
                    first_in[channel].at[step - 1],
                )
                copies[channel, step].start()
        return copies

    def passage_sums(channels, before, target):
        for channel in channels:
            _, first, units, turn = CHANNELS[channel]
            for step in STEPS:
                before[channel, step].wait()
            held = fewer[channel][coordinate(me, lines(turn)[0])].astype(jnp.float32)
            for step in STEPS:
                held = held + first_in[channel][step - 1].astype(jnp.float32)
            held = held.astype(jnp.bfloat16)
            for passage in range(PASS_DEV):
                for unit in range(units):
                    row, column = unit_place(first + unit)
                    target[pl.ds(passage * PLEN + row, 16), pl.ds(column, 128)] = held[
                        passage, unit
                    ]

    def near(at, source, target):
        return pltpu.make_async_remote_copy(
            src_ref=source,
            dst_ref=target,
            send_sem=near_send.at[at],
            recv_sem=near_recv.at[at],
            device_id={"tp": sibling},
            device_id_type=MESH,
        )

    length = dq.shape[0]
    part = length // 2

    def rows_of(left):
        return jnp.concatenate(
            [left[aligned(sibling * part, part), :], left[aligned(core * part, part), :]], axis=0
        )

    def token_grads(start, stop):
        @pl.loop(start, stop)
        def _(tile):
            columns = aligned(tile * 256, 256, 256)
            made = nt(rows_of(dq), w_q[columns, :])
            made = made + nt(rows_of(grq), w_rq[columns, :])
            made = made + nt(rows_of(grk), w_rk[columns, :])
            made = made + nt(rows_of(grv), w_rv[columns, :])
            theirs[tile] = made[:part].astype(jnp.bfloat16)
            mine[tile] = made[part:]
            near(tile, theirs.at[tile], passed.at[tile]).start()

    def token_ends(start, stop):
        @pl.loop(start, stop)
        def _(tile):
            near(tile, theirs.at[tile], passed.at[tile]).wait()
            columns = aligned(tile * 256, 256, 256)
            gt[:, columns] = (mine[tile] + passed[tile].astype(jnp.float32)).astype(
                jnp.bfloat16
            )

    whole = ((0, pl.ds(0, 4)),)
    lower, upper = ((0, pl.ds(0, 2)),), ((1, pl.ds(2, 2)),)
    keys = third_stage(KEY_CHANNELS, whole)
    values = third_stage(VALUE_CHANNELS, lower)
    for one in own_loads + loads:
        one.start()
    for one in loads[:8]:
        one.wait()
    token_grads(0, 2)
    for one in own_loads:
        one.wait()
    waiting, keys = keys, {}
    for channel in KEY_CHANNELS:
        add_readers((channel,), waiting, 0, 4)
        keys.update(second_stage((channel,), whole))
    more = third_stage(VALUE_CHANNELS, upper)
    loads[8].wait()
    flipped[...] = store[...].T
    token_grads(2, 4)
    add_readers(VALUE_CHANNELS, values, 0, 2)
    token_grads(4, 5)
    keys = first_stage(KEY_CHANNELS, keys)
    token_grads(5, 6)
    waiting, values = more, {}
    for channel in VALUE_CHANNELS:
        add_readers((channel,), waiting, 2, 4)
        values.update(second_stage((channel,), lower))
    passage_sums(KEY_CHANNELS, keys, key_grad)
    term[...] = nn(flipped[...], key_grad[...])
    half[...] = term[...].astype(jnp.bfloat16)

    def ar_copy(stage, place, step, dim, source, target):
        return pltpu.make_async_remote_copy(
            src_ref=source,
            dst_ref=target,
            send_sem=ar_send.at[stage, place, step - 1],
            recv_sem=ar_recv.at[stage, place, step - 1],
            device_id={"st": peer_of(me, dim, step)},
            device_id_type=MESH,
        )

    started = []
    for place, (start, size) in enumerate(PARTS):
        dim = lines(place)[0]
        at = coordinate(me, dim)
        quarter = size // 4
        for step in STEPS:
            there = lax.rem(at + step, 4)
            one = ar_copy(
                0,
                place,
                step,
                dim,
                half.at[aligned(start + there * quarter, quarter)],
                ar_first.at[step - 1, pl.ds(start // 4, quarter)],
            )
            one.start()
            started.append(one)
    values.update(second_stage(VALUE_CHANNELS, upper))
    token_grads(6, 8)
    for one in loads[9:]:
        one.wait()
    stage = []
    for place, (start, size) in enumerate(PARTS):
        dim, other, _ = lines(place)
        at, beside = coordinate(me, dim), coordinate(me, other)
        quarter, small = size // 4, size // 16
        base = start + at * quarter
        for step in STEPS:
            started[place * 3 + step - 1].wait()
        held = term[aligned(base, quarter), :]
        for step in STEPS:
            held = held + ar_first[step - 1, pl.ds(start // 4, quarter), :].astype(jnp.float32)
        total[pl.ds(start // 4, quarter), :] = held
        half[aligned(base, quarter), :] = held.astype(jnp.bfloat16)
        for step in STEPS:
            there = lax.rem(beside + step, 4)
            one = ar_copy(
                1,
                place,
                step,
                other,
                half.at[aligned(base + there * small, small)],
                ar_second.at[step - 1, pl.ds(start // 16, small)],
            )
            one.start()
            stage.append(one)
    values = first_stage(VALUE_CHANNELS, values)
    token_ends(0, 4)
    started, stage = stage, []
    for place, (start, size) in enumerate(PARTS):
        dim, other, last = lines(place)
        at, beside = coordinate(me, dim), coordinate(me, other)
        quarter, small = size // 4, size // 16
        base = start + at * quarter + beside * small
        for step in STEPS:
            started[place * 3 + step - 1].wait()
        held = total[aligned(start // 4 + beside * small, small), :]
        for step in STEPS:
            held = held + ar_second[step - 1, pl.ds(start // 16, small), :].astype(jnp.float32)
        half[aligned(base, small), :] = held.astype(jnp.bfloat16)
        for step in STEPS:
            one = ar_copy(
                2,
                place,
                step,
                last,
                half.at[aligned(base, small)],
                ar_third.at[step - 1, pl.ds(start // 16, small)],
            )
            one.start()
            stage.append(one)
    passage_sums(VALUE_CHANNELS, values, value_grad)
    store_rows = 2 * PLEN
    made = nt(
        jnp.concatenate(
            [
                key_grad[aligned(sibling * store_rows, store_rows), :],
                key_grad[aligned(core * store_rows, store_rows), :],
            ],
            axis=0,
        ),
        w_key[...],
    ) + nt(
        jnp.concatenate(
            [
                value_grad[aligned(sibling * store_rows, store_rows), :],
                value_grad[aligned(core * store_rows, store_rows), :],
            ],
            axis=0,
        ),
        w_value[...],
    )
    store_theirs[...] = made[:store_rows].astype(jnp.bfloat16)
    store_mine[...] = made[store_rows:]
    store_near = near(8, store_theirs, store_passed)
    store_near.start()
    token_ends(4, 8)
    ends = [pltpu.make_async_copy(gt, gt_any, load.at[17])]
    ends[0].start()
    started, stage = stage, []
    for place, (start, size) in enumerate(PARTS):
        dim, other, _ = lines(place)
        at, beside = coordinate(me, dim), coordinate(me, other)
        quarter, small = size // 4, size // 16
        base = start + at * quarter + beside * small
        for step in STEPS:
            started[place * 3 + step - 1].wait()
        rows = pl.ds(start // 16, small)
        held = half[aligned(base, small), :].astype(jnp.float32) + ar_third[1, rows, :].astype(
            jnp.float32
        )
        held = held + (
            ar_third[0, rows, :].astype(jnp.float32) + ar_third[2, rows, :].astype(jnp.float32)
        )
        out[aligned(base, small), :] = held.astype(jnp.bfloat16)
        for step in STEPS:
            here = out.at[aligned(base, small)]
            one = ar_copy(3, place, step, other, here, here)
            one.start()
            stage.append(one)
    store_near.wait()
    gs[...] = (store_mine[...] + store_passed[...].astype(jnp.float32)).astype(jnp.bfloat16)
    ends.append(pltpu.make_async_copy(gs, gs_any, load.at[18]))
    ends[1].start()
    started, stage = stage, []
    for place, (start, size) in enumerate(PARTS):
        dim = lines(place)[0]
        at = coordinate(me, dim)
        quarter = size // 4
        base = start + at * quarter
        for step in STEPS:
            started[place * 3 + step - 1].wait()
        for step in STEPS:
            here = out.at[aligned(base, quarter)]
            one = ar_copy(4, place, step, dim, here, here)
            one.start()
            stage.append(one)
    for one in stage + ends:
        one.wait()


def backward(
    need, asked, store, w_key, w_value, dq, grq, grk, grv, w_q, w_rq, w_rk, w_rv, leaving
):
    bf16, f32 = jnp.bfloat16, jnp.float32
    length, width = dq.shape[0], store.shape[1]
    units = [channel[2] for channel in CHANNELS]
    kv_width = w_key.shape[1]
    tiles = width // 256
    scratch = (
        [pltpu.VMEM((4, 4, n, 16, 128), bf16) for n in units]
        + [pltpu.VMEM((3, 4, 4, n, 16, 128), bf16) for n in units]
        + [pltpu.VMEM((4, 4, 4, n, 16, 128), bf16) for n in units]
        + [pltpu.VMEM((3, 4, 4, n, 16, 128), bf16) for n in units]
        + [pltpu.VMEM((4, 4, n, 16, 128), bf16) for n in units]
        + [pltpu.VMEM((3, 4, n, 16, 128), bf16) for n in units]
        + [
            pltpu.VMEM(array.shape, array.dtype)
            for array in (store, w_key, w_value, dq, grq, grk, grv, w_q, w_rq, w_rk, w_rv)
        ]
        + [
            pltpu.VMEM((tiles, length // 2, 256), f32),
            pltpu.VMEM((tiles, length // 2, 256), bf16),
            pltpu.VMEM((tiles, length // 2, 256), bf16),
            pltpu.VMEM((2 * PLEN, width), f32),
            pltpu.VMEM((2 * PLEN, width), bf16),
            pltpu.VMEM((2 * PLEN, width), bf16),
            pltpu.VMEM((PASS_DEV * PLEN, kv_width), bf16),
            pltpu.VMEM((PASS_DEV * PLEN, kv_width), bf16),
            pltpu.VMEM((width, kv_width), f32),
            pltpu.VMEM((width, kv_width), bf16),
            pltpu.VMEM((width // 4, kv_width), f32),
            pltpu.VMEM((3, width // 4, kv_width), bf16),
            pltpu.VMEM((3, width // 16, kv_width), bf16),
            pltpu.VMEM((3, width // 16, kv_width), bf16),
            pltpu.VMEM((length // 2, width), bf16),
            pltpu.VMEM((2 * PLEN, width), bf16),
            pltpu.VMEM((width, PASS_DEV * PLEN), bf16),
            pltpu.SemaphoreType.DMA((19,)),
            pltpu.SemaphoreType.DMA((9,)),
            pltpu.SemaphoreType.DMA((9,)),
            pltpu.SemaphoreType.DMA((3, 6, 3, 2)),
            pltpu.SemaphoreType.DMA((3, 6, 3, 2)),
            pltpu.SemaphoreType.DMA((5, 3, 3)),
            pltpu.SemaphoreType.DMA((5, 3, 3)),
        ]
    )
    return pl.pallas_call(
        backward_kernel,
        name="return_and_reduce",
        out_shape=[
            jax.ShapeDtypeStruct((length // 2, width), bf16),
            jax.ShapeDtypeStruct((2 * PLEN, width), bf16),
            jax.ShapeDtypeStruct((width, kv_width), bf16),
        ],
        in_specs=[smem_spec(), smem_spec()] + [any_spec()] * 17,
        out_specs=[any_spec(), any_spec(), vmem_spec()],
        scratch_shapes=scratch,
        compiler_params=pltpu.CompilerParams(
            collective_id=1, has_side_effects=True, vmem_limit_bytes=VMEM_LIMIT
        ),
    )(need, asked, store, w_key, w_value, dq, grq, grk, grv, w_q, w_rq, w_rk, w_rv, *leaving)


def finish_kernel(gt_in, gs_in, gw_in, gt_ref, gs_ref, gw_ref):
    gt_ref[...] = gt_in[...]
    gs_ref[...] = gs_in[...]
    gw_ref[...] = gw_in[...].astype(jnp.float32)


def finish(*arrays):
    steps = 4
    specs = [
        pl.BlockSpec((array.shape[0] // steps, array.shape[1]), lambda step: (step, 0))
        for array in arrays
    ]
    return pl.pallas_call(
        finish_kernel,
        name="finish",
        out_shape=[
            jax.ShapeDtypeStruct(array.shape, dtype)
            for array, dtype in zip(arrays, (jnp.bfloat16, jnp.bfloat16, jnp.float32))
        ],
        grid=(steps,),
        in_specs=specs,
        out_specs=specs,
    )(*arrays)


def per_device(
    tokens,
    store,
    passage_ids,
    w_query,
    w_key,
    w_value,
    w_ret_query,
    w_ret_key,
    w_ret_value,
    ret_rate,
    ret_gain,
    gate_logit,
    out_grad,
):
    width = store.shape[2]
    ids = passage_ids.reshape(-1)
    owners = jnp.arange(128, dtype=jnp.int32)
    need = jnp.sum(
        jnp.where(owners[:, None] == (ids // PASS_DEV)[None, :], (ids % PASS_DEV)[None, :], 0),
        axis=1,
    ).reshape(1, 1, 128)
    store_rows = store.reshape(-1, width)
    made = forward(
        need,
        ret_rate,
        ret_gain.reshape(1, -1),
        store_rows,
        w_key,
        w_value,
        tokens,
        w_ret_query,
        w_ret_key,
        w_ret_value,
        w_query,
        out_grad,
    )
    arrived, (asked, q, grq, grk, grv) = made[:6], made[6:]
    dq, leaving = attention(ids, gate_logit.reshape(1, -1), q, out_grad, arrived)
    made = backward(
        need,
        asked,
        store_rows,
        w_key,
        w_value,
        dq,
        grq,
        grk,
        grv,
        w_query,
        w_ret_query,
        w_ret_key,
        w_ret_value,
        leaving,
    )
    grad_tokens, grad_store, grad_key_weight = finish(*made)
    return (grad_tokens, grad_store.reshape(-1, PLEN, width), grad_key_weight)


def solution(mesh):
    return jax.shard_map(
        per_device,
        mesh=mesh,
        in_specs=(
            P("st", None),
            P("st", None, None),
            P("st", None),
            P(None, "tp"),
            P(None, "tp"),
            P(None, "tp"),
            P(None, "tp"),
            P(None, "tp"),
            P(None, "tp"),
            P("tp"),
            P("tp"),
            P("tp"),
            P("st", "tp"),
        ),
        out_specs=(P(("st", "tp"), None), P(("st", "tp"), None, None), P(None, "tp")),
        check_vma=False,
    )
```
